128 devices in a mesh: sp: 16 (over z, y), tp: 8 (over x, core).
Axes of the slice: x: 4, y: 4, z: 4, core: 2. Of those that a mesh axis runs over, the one named last changes fastest.
Arguments:
- residual: bfloat16 [10240, 2048], P('sp', 'tp'), may hold values from -4 to 4
- query_wide: bfloat16 [10240, 1536], P('sp', 'tp'), may hold values from -500 to 500
- query_narrow: bfloat16 [10240, 1024], P('sp', 'tp'), may hold values from -500 to 500
- latent: bfloat16 [10240, 512], P('sp'), may hold values from -6 to 6
- rope_key: bfloat16 [10240, 64], P('sp'), may hold values from -6 to 6
- latent_gain: float32 [512], replicated, may hold values from 0.1 to 1.9
- expand_wide: bfloat16 [512, 2048], P(None, 'tp'), may hold values from -0.25 to 0.25
- expand_narrow: bfloat16 [512, 1024], P(None, 'tp'), may hold values from -0.25 to 0.25
- out_wide: bfloat16 [1024, 2048], P('tp'), may hold values from -0.1875 to 0.1875
- out_narrow: bfloat16 [512, 2048], P('tp'), may hold values from -0.25 to 0.25
- norm_gain: float32 [2048], P('tp'), may hold values from 0.1 to 1.9
- up_gate: bfloat16 [2048, 5632], P('sp', 'tp'), may hold values from -0.125 to 0.125
- up_value: bfloat16 [2048, 5632], P('sp', 'tp'), may hold values from -0.125 to 0.125
- down_weight: bfloat16 [2048, 5632], P('sp', 'tp'), may hold values from -0.078125 to 0.078125
- conv_taps: float32 [3, 2, 5632], P(None, None, 'tp'), may hold values from -3 to 3
Outputs:
- output: bfloat16 [10240, 2048], P('sp', 'tp')
The draws below stay inside these ranges and needn't reach their ends.
All inputs are finite; a program needn't handle non-finite values.
Results may differ from the reference program's by a relative error of at most 0.025.
Values may be sent and summed in bfloat16 or wider, within the bound.
A program may use at most 192 MiB of HBM per device.

```python
import math
import jax
import jax.numpy as jnp
from jax import lax

D = 2048
FF = 5632
RANK = 512
ROPE = 64
HW = 8
NOPE_W = 128
VAL_W = 128
HN = 8
NOPE_N = 64
VAL_N = 64
TOKENS = 10240
N_TP = 8


def draw_residual(key, part):
    key_noise = jax.random.fold_in(key, 11)
    columns = jnp.arange(D, dtype=jnp.float32) / D
    values = jax.random.normal(key_noise, (TOKENS, D), jnp.float32) * 0.1 * jnp.exp(1.6 * columns)[None, :]
    return jnp.clip(values, -4.0, 4.0).astype(jnp.bfloat16)


def query_values(key, arr_shape):
    key_noise = jax.random.fold_in(key, 21)
    values = jax.random.normal(key_noise, arr_shape, jnp.float32) * 2.5
    return jnp.clip(values, -12.0, 12.0)


def draw_query_wide(key, part):
    return query_values(jax.random.fold_in(key, 1), (TOKENS, HW * (NOPE_W + ROPE))).astype(jnp.bfloat16)


def draw_query_narrow(key, part):
    return query_values(jax.random.fold_in(key, 2), (TOKENS, HN * (NOPE_N + ROPE))).astype(jnp.bfloat16)


def level_of(key, dims, cuts, smallest, high):
    gain = 1.0
    for dim, blocks in cuts:
        draws = jax.random.uniform(jax.random.fold_in(jax.random.fold_in(key, 6), dim), (blocks,), jnp.float32, smallest / len(cuts), high / len(cuts))
        gain = gain * jnp.repeat(jnp.exp(draws), dims[dim] // blocks).reshape((-1,) + (1,) * (len(dims) - 1 - dim))
    return gain


def scatter_about(key, extent, scale, reach, cuts=(), kind=jnp.bfloat16):
    level = level_of(key, extent, cuts, -0.22, 0.18) if cuts else 1.0
    values = jax.random.normal(key, extent, jnp.float32) * scale * level
    return jnp.minimum(jnp.maximum(values, -reach), reach).astype(kind)


def setup_inputs(seed: int = 0) -> dict:
    arg_keys = jax.random.split(jax.random.key(seed), 16)
    return {
        "residual": draw_residual(jax.random.fold_in(arg_keys[15], 71), 0),
        "query_wide": draw_query_wide(jax.random.fold_in(arg_keys[15], 71), 0),
        "query_narrow": draw_query_narrow(jax.random.fold_in(arg_keys[15], 71), 0),
        "latent": scatter_about(arg_keys[3], (TOKENS, RANK), 1.0, 6.0, ((0, 16),)),
        "rope_key": scatter_about(arg_keys[4], (TOKENS, ROPE), 1.0, 6.0, ((0, 16),)),
        "latent_gain": jnp.clip(1.0 + 0.18 * jax.random.normal(arg_keys[5], (RANK,), jnp.float32), 0.1, 1.9),
        "expand_wide": scatter_about(arg_keys[6], (RANK, HW * (NOPE_W + VAL_W)), RANK ** -0.5, 0.25, ((1, 8),)),
        "expand_narrow": scatter_about(arg_keys[7], (RANK, HN * (NOPE_N + VAL_N)), RANK ** -0.5, 0.25, ((1, 8),)),
        "out_wide": scatter_about(arg_keys[8], (HW * VAL_W, D), (HW * VAL_W) ** -0.5, 0.1875, ((0, 8),)),
        "out_narrow": scatter_about(arg_keys[9], (HN * VAL_N, D), (HN * VAL_N) ** -0.5, 0.25, ((0, 8),)),
        "norm_gain": jnp.clip(1.0 + 0.18 * jax.random.normal(arg_keys[10], (D,), jnp.float32), 0.1, 1.9),
        "up_gate": scatter_about(arg_keys[11], (D, FF), D ** -0.5, 0.125, ((0, 16), (1, 8))),
        "up_value": scatter_about(arg_keys[12], (D, FF), D ** -0.5, 0.125, ((0, 16), (1, 8))),
        "down_weight": scatter_about(arg_keys[13], (D, FF), FF ** -0.5, 0.078125, ((0, 16), (1, 8))),
        "conv_taps": scatter_about(arg_keys[14], (3, 2, FF), 0.6, 3.0, ((2, 8),), jnp.float32),
    }


theta = 10000.0
epsilon = 1e-06

def rotate(values, positions):
    half_dim = values.shape[-1] // 2
    inverse = jnp.power(jnp.float32(theta), -2.0 * jnp.arange(half_dim, dtype=jnp.float32) / values.shape[-1])
    angles = positions[:, None] * inverse[None, :]
    new_shape = (angles.shape[0],) + (1,) * (values.ndim - 2) + (half_dim,)
    cosine = jnp.cos(angles).reshape(new_shape)
    sine_part = jnp.sin(angles).reshape(new_shape)
    floats = values.astype(jnp.float32)
    lower_half = floats[..., :half_dim]
    upper_half = floats[..., half_dim:]
    turned = jnp.concatenate([lower_half * cosine - upper_half * sine_part, lower_half * sine_part + upper_half * cosine], axis=-1)
    return turned.astype(jnp.bfloat16)

def attend(query_turned, key_part, value_part, rope_turned, factor):
    nope_dim = key_part.shape[-1]
    head_count = query_turned.shape[1]
    block_rows = math.gcd(TOKENS, 512)
    grouped = query_turned.reshape(TOKENS // block_rows, block_rows, head_count, query_turned.shape[-1])
    key_float = key_part.astype(jnp.float32)
    rope_float = rope_turned.astype(jnp.float32)
    value_float = value_part.astype(jnp.float32)

    def one_block(query_block):
        query_float = query_block.astype(jnp.float32)
        scores = jnp.einsum('qhd,khd->hqk', query_float[..., :nope_dim], key_float)
        scores = (scores + jnp.einsum('qhd,kd->hqk', query_float[..., nope_dim:], rope_float)) * factor
        row_max = lax.optimization_barrier(jnp.max(scores, axis=-1, keepdims=True))
        weights = jnp.exp(scores - row_max)
        row_total = lax.optimization_barrier(jnp.sum(weights, axis=-1))
        rounded = lax.optimization_barrier(weights.astype(jnp.bfloat16)).astype(jnp.float32)
        weighted = jnp.einsum('hqk,khd->qhd', rounded, value_float)
        return (weighted / jnp.transpose(row_total)[:, :, None]).astype(jnp.bfloat16)
    outputs = lax.map(one_block, grouped)
    return outputs.reshape(TOKENS, head_count * value_part.shape[-1])

def turn_query(queries, head_count, nope_dim, positions):
    shaped = queries.reshape(TOKENS, head_count, nope_dim + ROPE)
    return jnp.concatenate([shaped[..., :nope_dim], rotate(shaped[..., nope_dim:], positions)], axis=-1)

def convolve(values, tap_rows):
    floats = values.astype(jnp.float32)
    zero_row = jnp.zeros((1, floats.shape[1]), jnp.float32)
    before = jnp.concatenate([zero_row, floats[:-1]], axis=0)
    after = jnp.concatenate([floats[1:], zero_row], axis=0)
    return tap_rows[0] * before + tap_rows[1] * floats + tap_rows[2] * after

def reference(residual, query_wide, query_narrow, latent, rope_key, latent_gain, expand_wide, expand_narrow, out_wide, out_narrow, norm_gain, up_gate, up_value, down_weight, conv_taps):
    positions = jnp.arange(TOKENS, dtype=jnp.int32).astype(jnp.float32)
    latent_float = latent.astype(jnp.float32)
    normed_latent = (latent_float * lax.rsqrt(lax.optimization_barrier(jnp.mean(latent_float * latent_float, axis=-1, keepdims=True)) + epsilon) * latent_gain).astype(jnp.bfloat16)
    rope_turned = rotate(rope_key, positions)
    kv_wide = jnp.dot(normed_latent, expand_wide, preferred_element_type=jnp.float32).astype(jnp.bfloat16).reshape(TOKENS, HW, NOPE_W + VAL_W)
    kv_narrow = jnp.dot(normed_latent, expand_narrow, preferred_element_type=jnp.float32).astype(jnp.bfloat16).reshape(TOKENS, HN, NOPE_N + VAL_N)
    query_w = turn_query(query_wide, HW, NOPE_W, positions)
    query_n = turn_query(query_narrow, HN, NOPE_N, positions)
    heads_wide = attend(query_w, kv_wide[..., :NOPE_W], kv_wide[..., NOPE_W:], rope_turned, (NOPE_W + ROPE) ** (-0.5))
    heads_narrow = attend(query_n, kv_narrow[..., :NOPE_N], kv_narrow[..., NOPE_N:], rope_turned, (NOPE_N + ROPE) ** (-0.5))
    wide_cols = HW // N_TP * VAL_W
    narrow_cols = HN // N_TP * VAL_N
    projected = jnp.zeros((TOKENS, D), jnp.float32)
    for group_index in range(N_TP):
        wide_slice = slice(group_index * wide_cols, (group_index + 1) * wide_cols)
        narrow_slice = slice(group_index * narrow_cols, (group_index + 1) * narrow_cols)
        partial_value = jnp.dot(heads_wide[:, wide_slice], out_wide[wide_slice], preferred_element_type=jnp.float32)
        partial_value = partial_value + jnp.dot(heads_narrow[:, narrow_slice], out_narrow[narrow_slice], preferred_element_type=jnp.float32)
        projected = projected + lax.optimization_barrier(partial_value.astype(jnp.bfloat16)).astype(jnp.float32)
    attended = (residual.astype(jnp.float32) + projected).astype(jnp.bfloat16)
    attended_float = attended.astype(jnp.float32)
    factor_rows = lax.rsqrt(lax.optimization_barrier(jnp.mean(attended_float * attended_float, axis=-1, keepdims=True)) + epsilon)
    normed = (attended_float * factor_rows * norm_gain).astype(jnp.bfloat16)
    gate_up = jnp.dot(normed, up_gate, preferred_element_type=jnp.float32).astype(jnp.bfloat16)
    value_up = jnp.dot(normed, up_value, preferred_element_type=jnp.float32).astype(jnp.bfloat16)
    hidden = (jax.nn.silu(convolve(gate_up, conv_taps[:, 0])) * convolve(value_up, conv_taps[:, 1])).astype(jnp.bfloat16)
    unit_cols = FF // N_TP
    channels = jnp.zeros((TOKENS, D), jnp.float32)
    for group_index in range(N_TP):
        unit_slice = slice(group_index * unit_cols, (group_index + 1) * unit_cols)
        partial_value = lax.dot_general(hidden[:, unit_slice], down_weight[:, unit_slice], (((1,), (1,)), ((), ())), preferred_element_type=jnp.float32)
        channels = channels + lax.optimization_barrier(partial_value.astype(jnp.bfloat16)).astype(jnp.float32)
    return (attended_float + channels).astype(jnp.bfloat16)
```

```python
import jax
import jax.numpy as jnp
from jax import lax
from jax.experimental import pallas as pl
from jax.experimental.pallas import tpu as pltpu
from jax.sharding import PartitionSpec as P

D = 2048
FF = 5632
RANK = 512
ROPE = 64
NOPE_W = 128
VAL_W = 128
NOPE_N = 64
VAL_N = 64
N_TP = 8
N_SP = 16
ROWS = 640
UNITS = FF // N_TP
FEATS = D // N_TP
EDGE = 16

theta = 10000.0
epsilon = 1e-06
LOG2E = 1.4426950408889634
SCALE_W = (NOPE_W + ROPE) ** -0.5 * LOG2E
SCALE_N = (NOPE_N + ROPE) ** -0.5 * LOG2E

MESH = pl.DeviceIdType.MESH
F32 = jnp.float32
BF16 = jnp.bfloat16

ORDER = (
    (0, 0), (1, 0), (3, 0), (0, 1), (0, 3), (2, 0), (1, 1), (1, 3),
    (3, 1), (3, 3), (0, 2), (2, 1), (2, 3), (1, 2), (3, 2), (2, 2),
)
SLOT = {offset: index for index, offset in enumerate(ORDER)}
PAIRS = len(ORDER) // 2
KEYS = 1280
CHUNK = 128


def rotate(values, positions):
    half_dim = values.shape[-1] // 2
    inverse = jnp.power(
        jnp.float32(theta), -2.0 * jnp.arange(half_dim, dtype=jnp.float32) / values.shape[-1]
    )
    angles = positions[:, None] * inverse[None, :]
    cosine = jnp.cos(angles)
    sine_part = jnp.sin(angles)
    floats = values.astype(jnp.float32)
    lower_half = floats[..., :half_dim]
    upper_half = floats[..., half_dim:]
    turned = jnp.concatenate(
        [
            lower_half * cosine - upper_half * sine_part,
            lower_half * sine_part + upper_half * cosine,
        ],
        axis=-1,
    )
    return turned.astype(jnp.bfloat16)


class Place:
    def __init__(self):
        self.sp = lax.axis_index("sp")
        self.tp = lax.axis_index("tp")
        self.z, self.y = lax.div(self.sp, 4), lax.rem(self.sp, 4)
        self.x, self.c = lax.div(self.tp, 2), lax.rem(self.tp, 2)

    def along(self, first, second):
        z = lax.rem(self.z + first * (1 - self.c) + second * self.c, 4)
        y = lax.rem(self.y + first * self.c + second * (1 - self.c), 4)
        return z * 4 + y

    def device(self, first, second):
        return {"sp": self.along(first, second), "tp": self.tp}

    def feature(self, dx, other=0):
        core = self.c if not other else 1 - self.c
        return lax.rem(self.x + dx, 4) * 2 + core

    def peer(self, dx, other=0):
        return {"sp": self.sp, "tp": self.feature(dx, other)}


class Copies:
    def __init__(self):
        self.sent = []

    def start(self, build):
        def copy():
            src, dst, send, recv, device = build()
            return pltpu.make_async_remote_copy(
                src_ref=src, dst_ref=dst, send_sem=send, recv_sem=recv, device_id=device, device_id_type=MESH
            )

        copy().start()
        self.sent.append(copy)

    def arrived(self, dst, recv, device):
        pltpu.make_async_remote_copy(
            src_ref=dst, dst_ref=dst, send_sem=recv, recv_sem=recv, device_id=device, device_id_type=MESH
        ).wait_recv()

    def drain(self):
        for copy in self.sent:
            copy().wait_send()
        self.sent = []


def onward(offset):
    df, ds = offset
    moves = []
    if ds == 0:
        if df == 3:
            moves.append((1, 0, 0, (2, 0)))
        if df == 1:
            moves.append((3, 0, 1, (2, 0)))
        if df == 0:
            moves.append((1, 0, None, (3, 0)))
            moves.append((3, 0, None, (1, 0)))
        moves.append((0, 1, None, (df, 3)))
        moves.append((0, 3, None, (df, 1)))
    elif ds == 3:
        moves.append((0, 1, 0, (df, 2)))
    elif ds == 1:
        moves.append((0, 3, 1, (df, 2)))
    return moves


MOVES = [(offset, move) for offset in ORDER for move in onward(offset)]
SEND = {key: index for index, key in enumerate(MOVES)}
N_SEND = len(MOVES)


class Gather:
    def __init__(self, copies, place, view, send, recv, own=None):
        self.copies, self.place, self.view = copies, place, view
        self.send, self.recv, self.own = send, recv, own

    def forward(self, offset):
        for move in onward(offset):
            for part in range(self.send.shape[0]):
                self.copies.start(lambda move=move, part=part: self._copy(offset, move, part))

    def _copy(self, offset, move, part):
        first, second, half, target = move
        source = self.own(half) if offset == (0, 0) and self.own else self.view(offset, half)
        return (
            source[part],
            self.landing(offset, target, half)[part],
            self.send.at[part, SEND[(offset, move)]],
            self.recv.at[part, SLOT[target] * 2 + (half or 0)],
            self.place.device(first, second),
        )

    def landing(self, offset, target, half):
        return self.view(target, half)

    def wait(self, offset):
        if offset == (0, 0):
            return
        halves = (0, 1) if 2 in offset and not (offset[0] == 2 and offset[1] in (1, 3)) else (None,)
        for half in halves:
            for part, dst in enumerate(self.view(offset, half)):
                self.copies.arrived(
                    dst, self.recv.at[part, SLOT[offset] * 2 + (half or 0)], self.place.device(0, 1)
                )


class GatherPlaced(Gather):
    def landing(self, offset, target, half):
        return self.view(offset, half)


class RingGather:
    def __init__(self, copies, place, view, send, recv):
        self.copies, self.place, self.view = copies, place, view
        self.send, self.recv = send, recv

    def _send(self, feature, half, index, arrival, device):
        for part, ref in enumerate(self.view(feature, half)):
            self.copies.start(
                lambda part=part, ref=ref: (ref, ref, self.send.at[part, index], self.recv.at[part, arrival], device)
            )

    def _wait(self, feature, half, arrival):
        for part, ref in enumerate(self.view(feature, half)):
            self.copies.arrived(ref, self.recv.at[part, arrival], self.place.peer(0, 1))

    def begin(self):
        place = self.place
        me = place.feature(0)
        self._send(me, None, 0, 0, place.peer(1))
        self._send(me, None, 1, 1, place.peer(3))
        self._send(me, None, 2, 4, place.peer(0, 1))

    def middle(self):
        place = self.place
        left, right = place.feature(3), place.feature(1)
        self._wait(left, None, 0)
        self._send(left, 0, 3, 2, place.peer(1))
        self._send(left, None, 4, 5, place.peer(0, 1))
        self._wait(right, None, 1)
        self._send(right, 1, 5, 3, place.peer(3))
        self._send(right, None, 6, 6, place.peer(0, 1))

    def end(self):
        place = self.place
        far = place.feature(2)
        self._wait(far, 0, 2)
        self._wait(far, 1, 3)
        self._send(far, None, 7, 7, place.peer(0, 1))
        self._wait(place.feature(0, 1), None, 4)
        self._wait(place.feature(3, 1), None, 5)
        self._wait(place.feature(1, 1), None, 6)
        self._wait(place.feature(2, 1), None, 7)


def half_rows(half, rows, start=0):
    if half is None:
        return pl.ds(start, rows)
    return pl.ds(start + half * (rows // 2), rows // 2)


def kernel(
    qw_ref, qn_ref, lat_ref, rope_ref, ew_ref, en_ref, res_ref, ow_ref, on_ref, gain_ref, up_ref, dn_ref, taps_ref,
    out_ref,
    latb, ropb, upf, dnf, kbuf, vbuf, mrow, lrow, acc, hw, hn, oww, ownr, own0, own1, gains, att, nrm, upx, hid,
    part, send_a, recv_a, send_b, recv_b, send_c, recv_c,
    ls, lr, lps, lpr, us, ur, ds_, dr, hs, hr, as_, ar, xs, xr, es, er, rs, rr,
):
    place = Place()
    copies = Copies()
    c, tp, sp = place.c, place.tp, place.sp

    barrier = pltpu.get_barrier_semaphore()
    talk = [place.device(f, s) for f, s in ((1, 0), (3, 0), (0, 1), (0, 3))]
    talk += [{"sp": sp, "tp": lax.rem(tp + d, N_TP)} for d in range(1, N_TP)]
    talk += [{"sp": lax.rem(sp + d, N_SP), "tp": tp} for d in (1, N_SP - 1)]
    for device in talk:
        pl.semaphore_signal(barrier, inc=1, device_id=device, device_id_type=MESH)
    pl.semaphore_wait(barrier, len(talk))

    lat_gather = Gather(
        copies,
        place,
        lambda offset, half: [
            latb.at[c, SLOT[offset], half_rows(half, 320)],
            ropb.at[c, SLOT[offset], half_rows(half, 160)],
        ],
        ls,
        lr,
        own=lambda half: [lat_ref.at[c, half_rows(half, 320)], rope_ref.at[c, half_rows(half, 160)]],
    )

    def up_view(offset, half):
        origin = place.along(*offset)
        return [upf.at[half_rows(half, 128, origin * 128)]]

    def dn_view(offset, half):
        origin = place.along(*offset)
        return [dnf.at[half_rows(half, 128, origin * 128)]]

    up_gather = GatherPlaced(copies, place, up_view, us, ur, own=lambda half: [up_ref.at[half_rows(half, 128)]])
    dn_gather = GatherPlaced(copies, place, dn_view, ds_, dr, own=lambda half: [dn_ref.at[half_rows(half, 128)]])

    lat_gather.forward((0, 0))

    def exchange(d, start):
        to, source = lax.rem(tp + d, N_TP), lax.rem(tp + N_TP - d, N_TP)
        arrays = (
            (ow_ref.at[:, pl.ds(pl.multiple_of(to * FEATS, FEATS), FEATS)], oww.at[tp], oww.at[source]),
            (on_ref.at[:, pl.ds(pl.multiple_of(to * FEATS, FEATS), FEATS)], ownr.at[tp], ownr.at[source]),
            (gain_ref, gains.at[tp], gains.at[source]),
        )
        for index, (src, dst, landed) in enumerate(arrays):
            if start:
                copies.start(
                    lambda src=src, dst=dst, index=index: (
                        src, dst, xs.at[index, d], xr.at[index, d], {"sp": sp, "tp": to}
                    )
                )
            else:
                copies.arrived(landed, xr.at[index, d], {"sp": sp, "tp": to})

    for d in range(1, N_TP):
        exchange(d, True)

    mine = pl.ds(pl.multiple_of(tp * FEATS, FEATS), FEATS)
    oww[tp] = ow_ref[:, mine]
    ownr[tp] = on_ref[:, mine]
    gains[tp] = gain_ref[...]
    upf[pl.ds(sp * 128, 128), :] = up_ref[...]
    dnf[pl.ds(sp * 128, 128), :] = dn_ref[...]
    for half in range(2):
        latb[half, 0] = lat_ref[half]
        ropb[half, 0] = rope_ref[half]

    mrow[...] = jnp.full_like(mrow, -1e30)
    lrow[...] = jnp.zeros_like(lrow)
    acc[...] = jnp.zeros_like(acc)

    def partner_view(core, slot):
        return [latb.at[core, slot], ropb.at[core, slot]]

    def attention_step(pair, carry):
        for k in range(PAIRS):

            @pl.when(pair == k)
            def _():
                for slot in (2 * k, 2 * k + 1):
                    offset = ORDER[slot]
                    if slot == 0:
                        continue
                    lat_gather.wait(offset)
                    lat_gather.forward(offset)
                    for index in range(2):
                        copies.start(
                            lambda index=index, slot=slot: (
                                partner_view(c, slot)[index], partner_view(c, slot)[index],
                                lps.at[index, slot], lpr.at[index, slot], place.peer(0, 1),
                            )
                        )
                if k == 6:
                    up_gather.forward((0, 0))
                if k == 7:
                    dn_gather.forward((0, 0))
                for slot in (2 * k, 2 * k + 1):
                    if slot:
                        for index, ref in enumerate(partner_view(1 - c, slot)):
                            copies.arrived(ref, lpr.at[index, slot], place.peer(0, 1))

        lane = lax.broadcasted_iota(jnp.int32, (160, 128), 1)
        for u in range(4):
            block = latb[u % 2, 2 * pair + u // 2]
            turned = ropb[u % 2, 2 * pair + u // 2].astype(F32)
            wide = jnp.dot(block, ew_ref[...], preferred_element_type=F32)
            narrow = jnp.dot(block, en_ref[...], preferred_element_type=F32)
            rows = pl.ds(u * 320, 320)
            kbuf[rows, 0:128] = wide[:, :128].astype(BF16)
            vbuf[rows, 0:128] = wide[:, 128:].astype(BF16)
            vbuf[rows, 128:256] = narrow.astype(BF16)
            kbuf[pl.ds(u * 320, 160), 128:256] = jnp.where(
                lane < 64, narrow[:160], pltpu.roll(turned, 64, 1)
            ).astype(BF16)
            kbuf[pl.ds(u * 320 + 160, 160), 128:256] = jnp.where(lane < 64, narrow[160:], turned).astype(BF16)

        def chunk_step(index, inner):
            for group in range(2):
                q_ref, lanes, scale = (qw_ref, slice(0, 256), SCALE_W) if group == 0 else (qn_ref, slice(128, 256), SCALE_N)
                q_rows = pl.ds(index * CHUNK, CHUNK)
                rows = pl.ds(group * ROWS + index * CHUNK, CHUNK)
                scores = lax.dot_general(
                    q_ref[q_rows, :], kbuf[:, lanes], (((1,), (1,)), ((), ())), preferred_element_type=F32
                )
                before = mrow[rows, 0:1]
                top = jnp.maximum(before, jnp.max(scores, axis=1, keepdims=True))
                weights = jnp.exp2((scores - top) * scale)
                shrink = jnp.exp2((before - top) * scale)
                total = shrink * lrow[rows, 0:1] + jnp.sum(weights, axis=1, keepdims=True)
                values = jnp.dot(
                    weights.astype(BF16), vbuf[:, group * 128 : group * 128 + 128], preferred_element_type=F32
                )
                acc[rows, :] = shrink * acc[rows, :] + values
                mrow[rows, :] = jnp.broadcast_to(top, (CHUNK, 128))
                lrow[rows, :] = jnp.broadcast_to(total, (CHUNK, 128))
            return inner

        lax.fori_loop(0, ROWS // CHUNK, chunk_step, 0)
        return carry

    lax.fori_loop(0, PAIRS, attention_step, 0)

    hw[tp] = (acc[0:ROWS, :] / lrow[0:ROWS, :]).astype(BF16)
    low = acc[ROWS : ROWS + 320, :] / lrow[ROWS : ROWS + 320, :]
    high = acc[ROWS + 320 : 2 * ROWS, :] / lrow[ROWS + 320 : 2 * ROWS, :]
    lane = lax.broadcasted_iota(jnp.int32, (320, 128), 1)
    hn[tp] = jnp.where(lane < 64, pltpu.roll(low, 64, 1), high).astype(BF16)
    head_gather = RingGather(
        copies,
        place,
        lambda feature, half: [hw.at[feature, half_rows(half, 640)], hn.at[feature, half_rows(half, 320)]],
        hs,
        hr,
    )
    head_gather.begin()

    for offset in ((1, 0), (3, 0), (0, 1), (0, 3)):
        up_gather.wait(offset)
        up_gather.forward(offset)

    for d in range(1, N_TP):
        exchange(d, False)
    zero = jnp.zeros((64, FEATS), BF16)
    for j in range(N_TP):
        own0[pl.ds(j * 128, 64), :] = ownr[j]
        own0[pl.ds(j * 128 + 64, 64), :] = zero
        own1[pl.ds(j * 128, 64), :] = zero
        own1[pl.ds(j * 128 + 64, 64), :] = ownr[j]

    head_gather.middle()
    for offset in ((2, 0), (1, 1), (1, 3), (3, 1), (3, 3)):
        up_gather.wait(offset)
        up_gather.forward(offset)
    for offset in ((1, 0), (3, 0), (0, 1), (0, 3)):
        dn_gather.wait(offset)
        dn_gather.forward(offset)
    head_gather.end()

    wide_heads = jnp.concatenate([hw[j] for j in range(N_TP)], axis=1)
    narrow_heads = jnp.concatenate([hn[j] for j in range(N_TP)], axis=1)
    summed = jnp.dot(wide_heads, oww[...].reshape(N_TP * 128, FEATS), preferred_element_type=F32)
    top = jnp.dot(narrow_heads, own0[...], preferred_element_type=F32)
    bottom = jnp.dot(narrow_heads, own1[...], preferred_element_type=F32)
    att[tp, 0:320] = (res_ref[0:320, :].astype(F32) + summed[0:320] + top).astype(BF16)
    att[tp, 320:640] = (res_ref[320:640, :].astype(F32) + summed[320:640] + bottom).astype(BF16)

    att_gather = RingGather(
        copies, place, lambda feature, half: [att.at[feature, half_rows(half, 640)]], as_, ar
    )
    att_gather.begin()
    for offset in ((0, 2), (2, 1), (2, 3)):
        up_gather.wait(offset)
        up_gather.forward(offset)
    att_gather.middle()
    for offset in ((1, 2), (3, 2), (2, 2)):
        up_gather.wait(offset)
        up_gather.forward(offset)
    for offset in ((2, 0), (1, 1), (1, 3), (3, 1), (3, 3)):
        dn_gather.wait(offset)
        dn_gather.forward(offset)
    att_gather.end()

    def norm_step(index, carry):
        rows = pl.ds(index * 64, 64)
        squares = jnp.zeros((64, FEATS), F32)
        for j in range(N_TP):
            piece = att[j, rows, :].astype(F32)
            squares = squares + piece * piece
        factor = lax.rsqrt(jnp.sum(squares, axis=1, keepdims=True) * (1.0 / D) + epsilon)
        for j in range(N_TP):
            nrm[rows, j * FEATS : (j + 1) * FEATS] = (
                att[j, rows, :].astype(F32) * factor * gains[j, 0:1, :]
            ).astype(BF16)
        return carry

    lax.fori_loop(0, ROWS // 64, norm_step, 0)

    def up_step(index, carry):
        columns = pl.ds(pl.multiple_of(index * 256, 256), 256)
        upx[EDGE : EDGE + ROWS, columns] = jnp.dot(
            nrm[...], upf[:, columns], preferred_element_type=F32
        ).astype(BF16)
        return carry

    lax.fori_loop(0, 5, up_step, 0)
    upx[EDGE : EDGE + ROWS, 1280:1408] = jnp.dot(nrm[...], upf[:, 1280:1408], preferred_element_type=F32).astype(BF16)

    following = {"sp": lax.rem(sp + 1, N_SP), "tp": tp}
    leading = {"sp": lax.rem(sp + N_SP - 1, N_SP), "tp": tp}
    copies.start(lambda: (upx.at[pl.ds(ROWS, EDGE)], upx.at[pl.ds(0, EDGE)], es.at[0], er.at[0], following))
    copies.start(lambda: (upx.at[pl.ds(EDGE, EDGE)], upx.at[pl.ds(ROWS + EDGE, EDGE)], es.at[1], er.at[1], leading))
    for offset in ((0, 2), (2, 1), (2, 3)):
        dn_gather.wait(offset)
        dn_gather.forward(offset)
    copies.arrived(upx.at[pl.ds(0, EDGE)], er.at[0], following)
    copies.arrived(upx.at[pl.ds(ROWS + EDGE, EDGE)], er.at[1], leading)

    def conv_step(index, carry):
        span = pl.ds(index * 128, 160)
        position = lax.broadcasted_iota(jnp.int32, (160, 1), 0) + index * 128 - EDGE
        outside = ((sp == 0) & (position < 0)) | ((sp == N_SP - 1) & (position >= ROWS))

        def smooth(columns):
            wide = jnp.where(outside, 0.0, upx[span, columns].astype(F32))
            low = pltpu.roll(wide, 1, 0)[16:144]
            high = pltpu.roll(wide, 159, 0)[16:144]
            return taps_ref[0:1, columns] * low + taps_ref[1:2, columns] * wide[16:144] + taps_ref[2:3, columns] * high

        def gated(gate, value):
            return gate / (1.0 + jnp.exp(-gate)) * value

        rows = pl.ds(index * 128, 128)
        for n in range(5):
            gate = smooth(slice(n * 128, n * 128 + 128))
            value = smooth(slice(640 + n * 128, 640 + n * 128 + 128))
            hid[rows, n * 128 : n * 128 + 128] = gated(gate, value).astype(BF16)
        both = smooth(slice(1280, 1408))
        hid[rows, 640:704] = gated(both, pltpu.roll(both, 64, 1))[:, :64].astype(BF16)
        return carry

    lax.fori_loop(0, 5, conv_step, 0)

    for offset in ((1, 2), (3, 2), (2, 2)):
        dn_gather.wait(offset)
        dn_gather.forward(offset)

    def down(feature):
        return lax.dot_general(
            hid[...], dnf[pl.ds(pl.multiple_of(feature * FEATS, FEATS), FEATS), :], (((1,), (1,)), ((), ())),
            preferred_element_type=F32,
        )

    for dx in (2, 1, 3, 0):
        send_a[dx] = down(place.feature(dx, 1)).astype(BF16)
        copies.start(lambda dx=dx: (send_a.at[dx], recv_a.at[dx], rs.at[dx], rr.at[dx], place.peer(0, 1)))
        part[dx] = down(place.feature(dx))

    def pair_sum(dx):
        copies.arrived(recv_a.at[dx], rr.at[dx], place.peer(0, 1))
        return part[dx] + recv_a[dx].astype(F32)

    far = pair_sum(2)
    send_b[0] = far[0:320].astype(BF16)
    send_b[1] = far[320:640].astype(BF16)
    copies.start(lambda: (send_b.at[0], recv_b.at[0], rs.at[4], rr.at[4], place.peer(1)))
    copies.start(lambda: (send_b.at[1], recv_b.at[1], rs.at[5], rr.at[5], place.peer(3)))
    right = pair_sum(1)
    left = pair_sum(3)
    send_c[0, 320:640] = right[320:640].astype(BF16)
    send_c[1, 0:320] = left[0:320].astype(BF16)
    copies.start(lambda: (send_c.at[0, pl.ds(320, 320)], recv_c.at[0, pl.ds(320, 320)], rs.at[6], rr.at[6], place.peer(1)))
    copies.start(lambda: (send_c.at[1, pl.ds(0, 320)], recv_c.at[1, pl.ds(0, 320)], rs.at[7], rr.at[7], place.peer(3)))
    copies.arrived(recv_b.at[0], rr.at[4], place.peer(1))
    send_c[0, 0:320] = (right[0:320] + recv_b[0].astype(F32)).astype(BF16)
    copies.start(lambda: (send_c.at[0, pl.ds(0, 320)], recv_c.at[0, pl.ds(0, 320)], rs.at[8], rr.at[8], place.peer(1)))
    copies.arrived(recv_b.at[1], rr.at[5], place.peer(3))
    send_c[1, 320:640] = (left[320:640] + recv_b[1].astype(F32)).astype(BF16)
    copies.start(lambda: (send_c.at[1, pl.ds(320, 320)], recv_c.at[1, pl.ds(320, 320)], rs.at[9], rr.at[9], place.peer(3)))
    own_sum = pair_sum(0) + att[tp].astype(F32)
    copies.arrived(recv_c.at[0, pl.ds(320, 320)], rr.at[6], place.peer(1))
    copies.arrived(recv_c.at[1, pl.ds(0, 320)], rr.at[7], place.peer(1))
    copies.arrived(recv_c.at[0, pl.ds(0, 320)], rr.at[8], place.peer(1))
    copies.arrived(recv_c.at[1, pl.ds(320, 320)], rr.at[9], place.peer(1))
    out_ref[...] = (own_sum + recv_c[0].astype(F32) + recv_c[1].astype(F32)).astype(BF16)
    copies.drain()


def per_device(
    residual, query_wide, query_narrow, latent, rope_key, latent_gain, expand_wide, expand_narrow,
    out_wide, out_narrow, norm_gain, up_gate, up_value, down_weight, conv_taps,
):
    offset = lax.axis_index("sp") * ROWS
    positions = (offset + lax.iota(jnp.int32, ROWS)).astype(jnp.float32)
    latent_float = latent.astype(jnp.float32)
    normed_latent = (
        latent_float
        * lax.rsqrt(jnp.mean(latent_float * latent_float, axis=-1, keepdims=True) + epsilon)
        * latent_gain
    ).astype(jnp.bfloat16)
    rope_turned = rotate(rope_key, positions)
    blank = jnp.zeros((ROWS, 64), BF16)
    q_wide = jnp.concatenate(
        [query_wide[:, :NOPE_W], blank, rotate(query_wide[:, NOPE_W:], positions)], axis=1
    )
    q_narrow = jnp.concatenate([query_narrow[:, :NOPE_N], rotate(query_narrow[:, NOPE_N:], positions)], axis=1)
    rope_packed = rope_turned.reshape(2, 2, 160, ROPE).transpose(0, 2, 1, 3).reshape(2, 160, 2 * ROPE)

    def interleave(gate, value):
        return jnp.concatenate(
            [gate[:, :640], value[:, :640], gate[:, 640:], value[:, 640:]], axis=1
        )

    up_block = interleave(up_gate, up_value)
    taps = interleave(conv_taps[:, 0], conv_taps[:, 1])
    gain = jnp.broadcast_to(norm_gain[None, :], (8, FEATS))
    vmem = pl.BlockSpec(memory_space=pltpu.VMEM)
    dma = pltpu.SemaphoreType.DMA
    return pl.pallas_call(
        kernel,
        out_shape=jax.ShapeDtypeStruct((ROWS, FEATS), BF16),
        in_specs=[vmem] * 13,
        out_specs=vmem,
        scratch_shapes=[
            pltpu.VMEM((2, 16, 320, RANK), BF16),
            pltpu.VMEM((2, 16, 160, 128), BF16),
            pltpu.VMEM((D, 2 * UNITS), BF16),
            pltpu.VMEM((D, UNITS), BF16),
            pltpu.VMEM((KEYS, 256), BF16),
            pltpu.VMEM((KEYS, 256), BF16),
            pltpu.VMEM((2 * ROWS, 128), F32),
            pltpu.VMEM((2 * ROWS, 128), F32),
            pltpu.VMEM((2 * ROWS, 128), F32),
            pltpu.VMEM((N_TP, ROWS, 128), BF16),
            pltpu.VMEM((N_TP, ROWS // 2, 128), BF16),
            pltpu.VMEM((N_TP, 128, FEATS), BF16),
            pltpu.VMEM((N_TP, 64, FEATS), BF16),
            pltpu.VMEM((N_TP * 128, FEATS), BF16),
            pltpu.VMEM((N_TP * 128, FEATS), BF16),
            pltpu.VMEM((N_TP, 8, FEATS), F32),
            pltpu.VMEM((N_TP, ROWS, FEATS), BF16),
            pltpu.VMEM((ROWS, D), BF16),
            pltpu.VMEM((ROWS + 2 * EDGE, 2 * UNITS), BF16),
            pltpu.VMEM((ROWS, UNITS), BF16),
            pltpu.VMEM((4, ROWS, FEATS), F32),
            pltpu.VMEM((4, ROWS, FEATS), BF16),
            pltpu.VMEM((4, ROWS, FEATS), BF16),
            pltpu.VMEM((2, ROWS // 2, FEATS), BF16),
            pltpu.VMEM((2, ROWS // 2, FEATS), BF16),
            pltpu.VMEM((2, ROWS, FEATS), BF16),
            pltpu.VMEM((2, ROWS, FEATS), BF16),
            dma((2, N_SEND)), dma((2, 32)), dma((2, 16)), dma((2, 16)),
            dma((1, N_SEND)), dma((1, 32)),
            dma((1, N_SEND)), dma((1, 32)),
            dma((2, 8)), dma((2, 8)),
            dma((1, 8)), dma((1, 8)),
            dma((3, 8)), dma((3, 8)),
            dma((2,)), dma((2,)),
            dma((10,)), dma((10,)),
        ],
        compiler_params=pltpu.CompilerParams(
            collective_id=0, has_side_effects=True, vmem_limit_bytes=67043328
        ),
    )(
        q_wide, q_narrow, normed_latent.reshape(2, 320, RANK), rope_packed, expand_wide, expand_narrow,
        residual, out_wide, out_narrow, gain, up_block, down_weight, taps,
    )


def solution(mesh):
    in_specs = (
        P("sp", "tp"), P("sp", "tp"), P("sp", "tp"), P("sp", None), P("sp", None), P(),
        P(None, "tp"), P(None, "tp"), P("tp", None), P("tp", None), P("tp"),
        P("sp", "tp"), P("sp", "tp"), P("sp", "tp"), P(None, None, "tp"),
    )
    return jax.shard_map(
        per_device, mesh=mesh, in_specs=in_specs, out_specs=P("sp", "tp"), check_vma=False
    )
```

```python
import jax
import jax.numpy as jnp
import numpy as np
from jax import lax
from jax.experimental import pallas as pl
from jax.experimental.pallas import tpu as pltpu
from jax.sharding import PartitionSpec as P

D = 2048
FF = 5632
RANK = 512
ROPE = 64
NOPE_W = 128
VAL_W = 128
NOPE_N = 64
VAL_N = 64
N_TP = 8
N_SP = 16
ROWS = 640
UNITS = FF // N_TP
FEATS = D // N_TP
EDGE = 16

theta = 10000.0
epsilon = 1e-06
LOG2E = 1.4426950408889634
SCALE_W = (NOPE_W + ROPE) ** -0.5 * LOG2E
SCALE_N = (NOPE_N + ROPE) ** -0.5 * LOG2E

MESH = pl.DeviceIdType.MESH
F32 = jnp.float32
BF16 = jnp.bfloat16

ORDER = (
    (0, 0), (1, 0), (3, 0), (0, 1), (0, 3), (2, 0), (1, 1), (1, 3),
    (3, 1), (3, 3), (0, 2), (2, 1), (2, 3), (1, 2), (3, 2), (2, 2),
)
SLOT = {offset: index for index, offset in enumerate(ORDER)}
PAIRS = len(ORDER) // 2
KEYS = 1280
CHUNK = 64
UP_START = 5
DN_START = 7


class Place:
    def __init__(self):
        self.sp = lax.axis_index("sp")
        self.tp = lax.axis_index("tp")
        self.z, self.y = lax.div(self.sp, 4), lax.rem(self.sp, 4)
        self.x, self.c = lax.div(self.tp, 2), lax.rem(self.tp, 2)

    def along(self, first, second):
        z = lax.rem(self.z + first * (1 - self.c) + second * self.c, 4)
        y = lax.rem(self.y + first * self.c + second * (1 - self.c), 4)
        return z * 4 + y

    def device(self, first, second):
        return {"sp": self.along(first, second), "tp": self.tp}

    def feature(self, dx, other=0):
        core = self.c if not other else 1 - self.c
        return lax.rem(self.x + dx, 4) * 2 + core

    def peer(self, dx, other=0):
        return {"sp": self.sp, "tp": self.feature(dx, other)}


class Copies:
    def __init__(self):
        self.sent = []

    def start(self, build):
        def copy():
            src, dst, send, recv, device = build()
            return pltpu.make_async_remote_copy(
                src_ref=src, dst_ref=dst, send_sem=send, recv_sem=recv, device_id=device, device_id_type=MESH
            )

        copy().start()
        self.sent.append(copy)

    def arrived(self, dst, recv, device):
        pltpu.make_async_remote_copy(
            src_ref=dst, dst_ref=dst, send_sem=recv, recv_sem=recv, device_id=device, device_id_type=MESH
        ).wait_recv()

    def drain(self):
        for copy in self.sent:
            copy().wait_send()
        self.sent = []


def onward(offset):
    df, ds = offset
    moves = []
    if ds == 0:
        if df == 3:
            moves.append((1, 0, 0, (2, 0)))
        if df == 1:
            moves.append((3, 0, 1, (2, 0)))
        if df == 0:
            moves.append((1, 0, None, (3, 0)))
            moves.append((3, 0, None, (1, 0)))
        moves.append((0, 1, None, (df, 3)))
        moves.append((0, 3, None, (df, 1)))
    elif ds == 3:
        moves.append((0, 1, 0, (df, 2)))
    elif ds == 1:
        moves.append((0, 3, 1, (df, 2)))
    return moves


MOVES = [(offset, move) for offset in ORDER for move in onward(offset)]
SEND = {key: index for index, key in enumerate(MOVES)}
N_SEND = len(MOVES)


class Gather:
    def __init__(self, copies, place, view, send, recv, own=None):
        self.copies, self.place, self.view = copies, place, view
        self.send, self.recv, self.own = send, recv, own

    def forward(self, offset):
        for move in onward(offset):
            for part in range(self.send.shape[0]):
                self.copies.start(lambda move=move, part=part: self._copy(offset, move, part))

    def _copy(self, offset, move, part):
        first, second, half, target = move
        source = self.own(half) if offset == (0, 0) and self.own else self.view(offset, half)
        return (
            source[part],
            self.landing(offset, target, half)[part],
            self.send.at[part, SEND[(offset, move)]],
            self.recv.at[part, SLOT[target] * 2 + (half or 0)],
            self.place.device(first, second),
        )

    def landing(self, offset, target, half):
        return self.view(target, half)

    def wait(self, offset):
        if offset == (0, 0):
            return
        halves = (0, 1) if 2 in offset and not (offset[0] == 2 and offset[1] in (1, 3)) else (None,)
        for half in halves:
            for part, dst in enumerate(self.view(offset, half)):
                self.copies.arrived(
                    dst, self.recv.at[part, SLOT[offset] * 2 + (half or 0)], self.place.device(0, 1)
                )


class GatherPlaced(Gather):
    def landing(self, offset, target, half):
        return self.view(offset, half)


class RingGather:
    def __init__(self, copies, place, view, send, recv):
        self.copies, self.place, self.view = copies, place, view
        self.send, self.recv = send, recv

    def _send(self, feature, half, index, arrival, device):
        for part, ref in enumerate(self.view(feature, half)):
            self.copies.start(
                lambda part=part, ref=ref: (ref, ref, self.send.at[part, index], self.recv.at[part, arrival], device)
            )

    def _wait(self, feature, half, arrival):
        for part, ref in enumerate(self.view(feature, half)):
            self.copies.arrived(ref, self.recv.at[part, arrival], self.place.peer(0, 1))

    def begin(self):
        place = self.place
        me = place.feature(0)
        self._send(me, None, 0, 0, place.peer(1))
        self._send(me, None, 1, 1, place.peer(3))
        self._send(me, None, 2, 4, place.peer(0, 1))

    def middle(self):
        place = self.place
        left, right = place.feature(3), place.feature(1)
        self._wait(left, None, 0)
        self._send(left, 0, 3, 2, place.peer(1))
        self._send(left, None, 4, 5, place.peer(0, 1))
        self._wait(right, None, 1)
        self._send(right, 1, 5, 3, place.peer(3))
        self._send(right, None, 6, 6, place.peer(0, 1))

    def end(self):
        place = self.place
        far = place.feature(2)
        self._wait(far, 0, 2)
        self._wait(far, 1, 3)
        self._send(far, None, 7, 7, place.peer(0, 1))
        self._wait(place.feature(0, 1), None, 4)
        self._wait(place.feature(3, 1), None, 5)
        self._wait(place.feature(1, 1), None, 6)
        self._wait(place.feature(2, 1), None, 7)


def half_rows(half, rows, start=0):
    if half is None:
        return pl.ds(start, rows)
    return pl.ds(start + half * (rows // 2), rows // 2)


def kernel(
    qw_hbm, qn_hbm, lat_hbm, rope_hbm, lgain_hbm, ew_hbm, en_hbm, res_hbm, ow_ref, on_ref, gain_ref, ug_ref, uv_ref, dn_ref,
    taps_hbm, inv_hbm, out_ref,
    latb, ropb, upf, dnf, kbuf, vbuf, sbuf, pbuf, mrow, acc, hw, hn, oww, ownr, own0, own1, gains, att, nrm, gx, vx, hid,
    part, send_a, recv_a, send_b, recv_b, send_c, recv_c,
    qt, qraw, qw_ref, qn_ref, lraw, rraw, lgain, ew_ref, en_ref, res_ref, taps_ref, inv_ref,
    ls, lr, lps, lpr, us, ur, ds_, dr, hs, hr, as_, ar, xs, xr, es, er, rs, rr, local,
):
    place = Place()
    copies = Copies()
    c, tp, sp = place.c, place.tp, place.sp

    mine = pl.ds(pl.multiple_of(tp * FEATS, FEATS), FEATS)
    loads = [
        (lat_hbm, lraw), (rope_hbm, rraw), (lgain_hbm, lgain), (inv_hbm, inv_ref), (qw_hbm, qt), (qn_hbm, qraw),
        (ew_hbm, ew_ref), (en_hbm, en_ref), (ug_ref, upf.at[sp, 0:UNITS]), (uv_ref, upf.at[sp, UNITS : 2 * UNITS]),
        (dn_ref, dnf.at[sp]), (ow_ref.at[:, mine], oww.at[tp]), (on_ref.at[:, mine], ownr.at[tp]),
        (gain_ref, gains.at[tp]), (res_hbm, res_ref), (taps_hbm, taps_ref),
    ]

    def load(index):
        src, dst = loads[index]
        return pltpu.make_async_copy(src, dst, local.at[index])

    for index in range(len(loads)):
        load(index).start()

    barrier = pltpu.get_barrier_semaphore()
    talk = [place.device(f, s) for f, s in ((1, 0), (3, 0), (0, 1), (0, 3))]
    talk += [{"sp": sp, "tp": lax.rem(tp + d, N_TP)} for d in range(1, N_TP)]
    talk += [{"sp": lax.rem(sp + d, N_SP), "tp": tp} for d in (1, N_SP - 1)]
    for device in talk:
        pl.semaphore_signal(barrier, inc=1, device_id=device, device_id_type=MESH)

    for index in range(4):
        load(index).wait()
    for half in range(2):
        floats = lraw[half * 320 : half * 320 + 320, :].astype(F32)
        mean = jnp.sum(floats * floats, axis=1, keepdims=True) * (1.0 / RANK)
        latb[half, 0] = (floats * lax.rsqrt(mean + epsilon) * lgain[...]).astype(BF16)
    position = (lax.broadcasted_iota(jnp.int32, (32, ROWS), 1) + sp * ROWS).astype(F32)
    angles = position * inv_ref[:, 0:1]
    cosine, sine = jnp.cos(angles), jnp.sin(angles)

    def turn(floats):
        lower, upper = floats[0:32], floats[32:64]
        return [lower * cosine - upper * sine, lower * sine + upper * cosine]

    turned = turn(rraw[...].astype(F32))
    doubled = jnp.transpose(jnp.concatenate(turned + turned, axis=0))
    lane = lax.broadcasted_iota(jnp.int32, (160, 128), 1)
    for half in range(2):
        start = half * 320
        ropb[half, 0] = jnp.where(lane < 64, doubled[start : start + 160], doubled[start + 160 : start + 320]).astype(BF16)

    pl.semaphore_wait(barrier, len(talk))

    lat_gather = Gather(
        copies,
        place,
        lambda offset, half: [
            latb.at[c, SLOT[offset], half_rows(half, 320)],
            ropb.at[c, SLOT[offset], half_rows(half, 160)],
        ],
        ls,
        lr,
    )

    def up_view(offset, half):
        return [upf.at[place.along(*offset), half_rows(half, 2 * UNITS)]]

    def dn_view(offset, half):
        return [dnf.at[place.along(*offset), half_rows(half, UNITS)]]

    up_gather = GatherPlaced(copies, place, up_view, us, ur)
    dn_gather = GatherPlaced(copies, place, dn_view, ds_, dr)

    lat_gather.forward((0, 0))

    def exchange(d, start):
        to, source = lax.rem(tp + d, N_TP), lax.rem(tp + N_TP - d, N_TP)
        theirs = pl.ds(pl.multiple_of(to * FEATS, FEATS), FEATS)
        arrays = (
            (ow_ref.at[:, theirs], oww.at[tp], oww.at[source]),
            (on_ref.at[:, theirs], ownr.at[tp], ownr.at[source]),
            (gain_ref, gains.at[tp], gains.at[source]),
        )
        for index, (src, dst, landed) in enumerate(arrays):
            if start:
                copies.start(
                    lambda src=src, dst=dst, index=index: (
                        src, dst, xs.at[index, d], xr.at[index, d], {"sp": sp, "tp": to}
                    )
                )
            else:
                copies.arrived(landed, xr.at[index, d], {"sp": sp, "tp": to})

    for d in range(1, N_TP):
        exchange(d, True)

    for index in (4, 5):
        load(index).wait()
    blank = jnp.zeros((64, ROWS), F32)
    rope_part = [SCALE_W * piece for piece in turn(qt[128:192, :].astype(F32))]
    qw_ref[:, 0:128] = jnp.transpose(qt[0:128, :].astype(F32)).astype(BF16)
    qw_ref[:, 128:256] = jnp.transpose(jnp.concatenate([blank] + rope_part, axis=0)).astype(BF16)
    narrow_query = jnp.transpose(qraw[...].astype(F32))
    rope_part = [SCALE_N * piece for piece in turn(narrow_query[64:128])]
    qn_ref[...] = jnp.transpose(jnp.concatenate([narrow_query[0:64]] + rope_part, axis=0)).astype(BF16)
    for index in (6, 7):
        load(index).wait()

    mrow[...] = jnp.full_like(mrow, -1e30)
    acc[...] = jnp.zeros_like(acc)

    def partner_view(core, slot):
        return [latb.at[core, slot], ropb.at[core, slot]]

    def own_arrivals(k):
        for slot in (2 * k, 2 * k + 1):
            if slot == 0:
                continue
            lat_gather.wait(ORDER[slot])
            lat_gather.forward(ORDER[slot])
            for index in range(2):
                copies.start(
                    lambda index=index, slot=slot: (
                        partner_view(c, slot)[index], partner_view(c, slot)[index],
                        lps.at[index, slot], lpr.at[index, slot], place.peer(0, 1),
                    )
                )
        if k == UP_START:
            for index in (8, 9):
                load(index).wait()
            up_gather.forward((0, 0))
        if k == DN_START:
            load(10).wait()
            dn_gather.forward((0, 0))

    def partner_arrivals(k):
        for slot in (2 * k, 2 * k + 1):
            if slot:
                for index, ref in enumerate(partner_view(1 - c, slot)):
                    copies.arrived(ref, lpr.at[index, slot], place.peer(0, 1))

    def expand(pair, side):
        lane = lax.broadcasted_iota(jnp.int32, (160, 128), 1)
        for u in range(4):
            block = latb[u % 2, 2 * pair + u // 2]
            rope = ropb[u % 2, 2 * pair + u // 2].astype(F32)
            wide = jnp.dot(block, ew_ref[...], preferred_element_type=F32)
            narrow = jnp.dot(block, en_ref[...], preferred_element_type=F32)
            rows = pl.ds(u * 320, 320)
            kbuf[side, rows, 0:128] = (wide[:, :128] * SCALE_W).astype(BF16)
            vbuf[side, rows, 0:128] = wide[:, 128:].astype(BF16)
            scaled = narrow * SCALE_N
            kbuf[side, pl.ds(u * 320, 160), 128:256] = jnp.where(
                lane < 64, scaled[:160], pltpu.roll(rope, 64, 1)
            ).astype(BF16)
            kbuf[side, pl.ds(u * 320 + 160, 160), 128:256] = jnp.where(lane < 64, scaled[160:], rope).astype(BF16)
            for row in (0, 160):
                vbuf[side, pl.ds(u * 320 + row, 160), 128:256] = jnp.where(lane < 64, 1.0, narrow[row : row + 160]).astype(
                    BF16
                )

    def score(group, side):
        q_ref, lanes = (qw_ref, slice(0, 256)) if group == 0 else (qn_ref, slice(128, 256))
        sbuf[group] = lax.dot_general(
            q_ref[...], kbuf[side, :, lanes], (((1,), (1,)), ((), ())), preferred_element_type=F32
        )

    def soften(group):
        for start in range(0, ROWS, CHUNK):
            rows = slice(start, start + CHUNK)
            kept = slice(group * ROWS + start, group * ROWS + start + CHUNK)
            scores = sbuf[group, rows, :]
            before = mrow[kept, :]
            top = jnp.maximum(before, jnp.max(scores, axis=1, keepdims=True))
            mrow[kept, :] = top
            pbuf[group, rows, :] = jnp.exp2(scores - top[:, 0:1]).astype(BF16)
            shrink = jnp.exp2(before - top)
            acc[kept, 0:128] = shrink * acc[kept, 0:128]
            if group == 0:
                acc[kept, 128:256] = shrink * acc[kept, 128:256]

    def gain_values(group, side):
        if group == 0:
            acc[0:ROWS, :] += jnp.dot(pbuf[0], vbuf[side], preferred_element_type=F32)
        else:
            acc[ROWS : 2 * ROWS, 0:128] += jnp.dot(pbuf[1], vbuf[side, :, 128:256], preferred_element_type=F32)

    own_arrivals(0)
    partner_arrivals(0)
    expand(0, 0)
    score(0, 0)

    def attention_step(pair, carry):
        side = lax.rem(pair, 2)
        for k in range(1, PAIRS):

            @pl.when(pair == k - 1)
            def _():
                own_arrivals(k)

        score(1, side)
        soften(0)
        gain_values(0, side)
        for k in range(1, PAIRS):

            @pl.when(pair == k - 1)
            def _():
                partner_arrivals(k)

        expand(pair + 1, 1 - side)
        score(0, 1 - side)
        soften(1)
        gain_values(1, side)
        return carry

    lax.fori_loop(0, PAIRS - 1, attention_step, 0)
    last = (PAIRS - 1) % 2
    score(1, last)
    soften(0)
    gain_values(0, last)
    soften(1)
    gain_values(1, last)

    hw[tp] = (acc[0:ROWS, 0:128] / acc[0:ROWS, 128:129]).astype(BF16)
    low = acc[ROWS : ROWS + 320, 0:128] / acc[ROWS : ROWS + 320, 0:1]
    high = acc[ROWS + 320 : 2 * ROWS, 0:128] / acc[ROWS + 320 : 2 * ROWS, 0:1]
    lane = lax.broadcasted_iota(jnp.int32, (320, 128), 1)
    hn[tp] = jnp.where(lane < 64, pltpu.roll(low, 64, 1), high).astype(BF16)
    head_gather = RingGather(
        copies,
        place,
        lambda feature, half: [hw.at[feature, half_rows(half, 640)], hn.at[feature, half_rows(half, 320)]],
        hs,
        hr,
    )
    head_gather.begin()

    for offset in ((1, 0), (3, 0), (0, 1), (0, 3)):
        up_gather.wait(offset)
        up_gather.forward(offset)

    for d in range(1, N_TP):
        exchange(d, False)
    for index in range(11, 16):
        load(index).wait()
    zero = jnp.zeros((64, FEATS), BF16)
    for j in range(N_TP):
        own0[pl.ds(j * 128, 64), :] = ownr[j]
        own0[pl.ds(j * 128 + 64, 64), :] = zero
        own1[pl.ds(j * 128, 64), :] = zero
        own1[pl.ds(j * 128 + 64, 64), :] = ownr[j]

    head_gather.middle()
    for offset in ((2, 0), (1, 1), (1, 3), (3, 1), (3, 3)):
        up_gather.wait(offset)
        up_gather.forward(offset)
    for offset in ((1, 0), (3, 0), (0, 1), (0, 3)):
        dn_gather.wait(offset)
        dn_gather.forward(offset)
    head_gather.end()

    wide_heads = jnp.concatenate([hw[j] for j in range(N_TP)], axis=1)
    narrow_heads = jnp.concatenate([hn[j] for j in range(N_TP)], axis=1)
    summed = jnp.dot(wide_heads, oww[...].reshape(N_TP * 128, FEATS), preferred_element_type=F32)
    top = jnp.dot(narrow_heads, own0[...], preferred_element_type=F32)
    bottom = jnp.dot(narrow_heads, own1[...], preferred_element_type=F32)
    att[tp, 0:320] = (res_ref[0:320, :].astype(F32) + summed[0:320] + top).astype(BF16)
    att[tp, 320:640] = (res_ref[320:640, :].astype(F32) + summed[320:640] + bottom).astype(BF16)

    att_gather = RingGather(
        copies, place, lambda feature, half: [att.at[feature, half_rows(half, 640)]], as_, ar
    )
    att_gather.begin()
    for offset in ((0, 2), (2, 1), (2, 3)):
        up_gather.wait(offset)
        up_gather.forward(offset)
    att_gather.middle()
    for offset in ((1, 2), (3, 2), (2, 2)):
        up_gather.wait(offset)
        up_gather.forward(offset)
    for offset in ((2, 0), (1, 1), (1, 3), (3, 1), (3, 3)):
        dn_gather.wait(offset)
        dn_gather.forward(offset)
    att_gather.end()

    def norm_step(index, carry):
        rows = pl.ds(index * 64, 64)
        squares = jnp.zeros((64, FEATS), F32)
        for j in range(N_TP):
            piece = att[j, rows, :].astype(F32)
            squares = squares + piece * piece
        factor = lax.rsqrt(jnp.sum(squares, axis=1, keepdims=True) * (1.0 / D) + epsilon)
        for j in range(N_TP):
            nrm[rows, j * FEATS : (j + 1) * FEATS] = (
                att[j, rows, :].astype(F32) * factor * gains[j]
            ).astype(BF16)
        return carry

    lax.fori_loop(0, ROWS // 64, norm_step, 0)

    for base, dest in ((0, gx), (UNITS, vx)):
        for start in (0, 256, 512):
            stop = min(start + 256, UNITS)
            weights = jnp.concatenate([upf[o, base + start : base + stop, :] for o in range(N_SP)], axis=1)
            dest[EDGE : EDGE + ROWS, start:stop] = lax.dot_general(
                nrm[...], weights, (((1,), (1,)), ((), ())), preferred_element_type=F32
            ).astype(BF16)

    following = {"sp": lax.rem(sp + 1, N_SP), "tp": tp}
    leading = {"sp": lax.rem(sp + N_SP - 1, N_SP), "tp": tp}
    edges = [
        (rows, landing, 2 * index + side, device)
        for side, (rows, landing, device) in enumerate(((ROWS, 0, following), (EDGE, ROWS + EDGE, leading)))
        for index in range(2)
    ]

    def edge(rows, landing, index, device):
        ref = (gx, vx)[index // 2]
        return ref.at[pl.ds(rows, EDGE)], ref.at[pl.ds(landing, EDGE)], es.at[index], er.at[index], device

    for entry in edges:
        copies.start(lambda entry=entry: edge(*entry))
    for offset in ((0, 2), (2, 1), (2, 3)):
        dn_gather.wait(offset)
        dn_gather.forward(offset)
    for rows, landing, index, device in edges:
        copies.arrived(edge(rows, landing, index, device)[1], er.at[index], device)

    def conv_step(index, carry):
        span = pl.ds(index * 128, 160)
        position = lax.broadcasted_iota(jnp.int32, (160, 1), 0) + index * 128 - EDGE
        outside = ((sp == 0) & (position < 0)) | ((sp == N_SP - 1) & (position >= ROWS))

        def smooth(ref, which, columns):
            wide = jnp.where(outside, 0.0, ref[span, columns].astype(F32))
            low = pltpu.roll(wide, 1, 0)[16:144]
            high = pltpu.roll(wide, 159, 0)[16:144]
            taps = [taps_ref[k, which : which + 1, columns] for k in range(3)]
            return taps[0] * low + taps[1] * wide[16:144] + taps[2] * high

        rows = pl.ds(index * 128, 128)
        for start in range(0, UNITS, 128):
            columns = slice(start, min(start + 128, UNITS))
            gate = smooth(gx, 0, columns)
            value = smooth(vx, 1, columns)
            hid[rows, columns] = (gate / (1.0 + jnp.exp(-gate)) * value).astype(BF16)
        return carry

    lax.fori_loop(0, 5, conv_step, 0)

    for offset in ((1, 2), (3, 2), (2, 2)):
        dn_gather.wait(offset)
        dn_gather.forward(offset)

    def down(feature):
        weights = jnp.concatenate([dnf[2 * feature], dnf[2 * feature + 1]], axis=1)
        return jnp.dot(hid[...], weights, preferred_element_type=F32)

    def down_pair(dx):
        send_a[dx] = down(place.feature(dx, 1)).astype(BF16)
        copies.start(lambda: (send_a.at[dx], recv_a.at[dx], rs.at[dx], rr.at[dx], place.peer(0, 1)))
        part[dx] = down(place.feature(dx))

    def pair_sum(dx):
        copies.arrived(recv_a.at[dx], rr.at[dx], place.peer(0, 1))
        return part[dx] + recv_a[dx].astype(F32)

    def send_half(side, index, dx):
        rows = pl.ds(320 * (index % 2), 320)
        copies.start(
            lambda: (send_c.at[side, rows], recv_c.at[side, rows], rs.at[6 + index], rr.at[6 + index], place.peer(dx))
        )

    down_pair(2)
    down_pair(1)
    far = pair_sum(2)
    send_b[0] = far[0:320].astype(BF16)
    copies.start(lambda: (send_b.at[0], recv_b.at[0], rs.at[4], rr.at[4], place.peer(1)))
    send_b[1] = far[320:640].astype(BF16)
    copies.start(lambda: (send_b.at[1], recv_b.at[1], rs.at[5], rr.at[5], place.peer(3)))
    down_pair(3)
    right = pair_sum(1)
    send_c[0, 320:640] = right[320:640].astype(BF16)
    send_half(0, 1, 1)
    part[1, 0:320] = right[0:320]
    down_pair(0)
    left = pair_sum(3)
    send_c[1, 0:320] = left[0:320].astype(BF16)
    send_half(1, 2, 3)
    copies.arrived(recv_b.at[0], rr.at[4], place.peer(1))
    send_c[0, 0:320] = (part[1, 0:320] + recv_b[0].astype(F32)).astype(BF16)
    send_half(0, 0, 1)
    copies.arrived(recv_b.at[1], rr.at[5], place.peer(3))
    send_c[1, 320:640] = (left[320:640] + recv_b[1].astype(F32)).astype(BF16)
    send_half(1, 3, 3)
    own_sum = pair_sum(0) + att[tp].astype(F32)
    for side, index in ((0, 1), (1, 2), (0, 0), (1, 3)):
        copies.arrived(recv_c.at[side, pl.ds(320 * (index % 2), 320)], rr.at[6 + index], place.peer(1))
    out_ref[...] = (own_sum + recv_c[0].astype(F32) + recv_c[1].astype(F32)).astype(BF16)
    copies.drain()


def per_device(
    residual, query_wide, query_narrow, latent, rope_key, latent_gain, expand_wide, expand_narrow,
    out_wide, out_narrow, norm_gain, up_gate, up_value, down_weight, conv_taps,
):
    inverse = np.power(np.float32(theta), -2.0 * np.arange(32, dtype=np.float32) / ROPE).astype(np.float32)
    inverse = jnp.asarray(np.broadcast_to(inverse[:, None], (32, 128)))
    vmem = pl.BlockSpec(memory_space=pltpu.VMEM)
    anywhere = pl.BlockSpec(memory_space=pl.ANY)
    dma = pltpu.SemaphoreType.DMA
    return pl.pallas_call(
        kernel,
        out_shape=jax.ShapeDtypeStruct((ROWS, FEATS), BF16),
        in_specs=[anywhere] * 16,
        out_specs=vmem,
        scratch_shapes=[
            pltpu.VMEM((2, 16, 320, RANK), BF16),
            pltpu.VMEM((2, 16, 160, 128), BF16),
            pltpu.VMEM((N_SP, 2 * UNITS, 128), BF16),
            pltpu.VMEM((N_SP, UNITS, 128), BF16),
            pltpu.VMEM((2, KEYS, 256), BF16),
            pltpu.VMEM((2, KEYS, 256), BF16),
            pltpu.VMEM((2, ROWS, KEYS), F32),
            pltpu.VMEM((2, ROWS, KEYS), BF16),
            pltpu.VMEM((2 * ROWS, 128), F32),
            pltpu.VMEM((2 * ROWS, 256), F32),
            pltpu.VMEM((N_TP, ROWS, 128), BF16),
            pltpu.VMEM((N_TP, ROWS // 2, 128), BF16),
            pltpu.VMEM((N_TP, 128, FEATS), BF16),
            pltpu.VMEM((N_TP, 64, FEATS), BF16),
            pltpu.VMEM((N_TP * 128, FEATS), BF16),
            pltpu.VMEM((N_TP * 128, FEATS), BF16),
            pltpu.VMEM((N_TP, 1, FEATS), F32),
            pltpu.VMEM((N_TP, ROWS, FEATS), BF16),
            pltpu.VMEM((ROWS, D), BF16),
            pltpu.VMEM((ROWS + 2 * EDGE, UNITS), BF16),
            pltpu.VMEM((ROWS + 2 * EDGE, UNITS), BF16),
            pltpu.VMEM((ROWS, UNITS), BF16),
            pltpu.VMEM((4, ROWS, FEATS), F32),
            pltpu.VMEM((4, ROWS, FEATS), BF16),
            pltpu.VMEM((4, ROWS, FEATS), BF16),
            pltpu.VMEM((2, ROWS // 2, FEATS), BF16),
            pltpu.VMEM((2, ROWS // 2, FEATS), BF16),
            pltpu.VMEM((2, ROWS, FEATS), BF16),
            pltpu.VMEM((2, ROWS, FEATS), BF16),
            pltpu.VMEM((NOPE_W + ROPE, ROWS), BF16),
            pltpu.VMEM((ROWS, 128), BF16),
            pltpu.VMEM((ROWS, 256), BF16),
            pltpu.VMEM((ROWS, 128), BF16),
            pltpu.VMEM((ROWS, RANK), BF16),
            pltpu.VMEM((ROPE, ROWS), BF16),
            pltpu.VMEM((1, RANK), F32),
            pltpu.VMEM((RANK, 256), BF16),
            pltpu.VMEM((RANK, 128), BF16),
            pltpu.VMEM((ROWS, FEATS), BF16),
            pltpu.VMEM((3, 2, UNITS), F32),
            pltpu.VMEM((32, 128), F32),
            dma((2, N_SEND)), dma((2, 32)), dma((2, 16)), dma((2, 16)),
            dma((1, N_SEND)), dma((1, 32)),
            dma((1, N_SEND)), dma((1, 32)),
            dma((2, 8)), dma((2, 8)),
            dma((1, 8)), dma((1, 8)),
            dma((3, 8)), dma((3, 8)),
            dma((4,)), dma((4,)),
            dma((10,)), dma((10,)),
            dma((16,)),
        ],
        compiler_params=pltpu.CompilerParams(
            collective_id=0, has_side_effects=True, vmem_limit_bytes=67043328
        ),
    )(
        query_wide.T, query_narrow, latent, rope_key.T, latent_gain.reshape(1, RANK), expand_wide, expand_narrow,
        residual, out_wide, out_narrow, norm_gain.reshape(1, FEATS), up_gate.T, up_value.T, down_weight.T, conv_taps, inverse,
    )


def solution(mesh):
    in_specs = (
        P("sp", "tp"), P("sp", "tp"), P("sp", "tp"), P("sp", None), P("sp", None), P(),
        P(None, "tp"), P(None, "tp"), P("tp", None), P("tp", None), P("tp"),
        P("sp", "tp"), P("sp", "tp"), P("sp", "tp"), P(None, None, "tp"),
    )
    return jax.shard_map(
        per_device, mesh=mesh, in_specs=in_specs, out_specs=P("sp", "tp"), check_vma=False
    )
```

```python
import jax
import jax.numpy as jnp
import numpy as np
from jax import lax
from jax.experimental import pallas as pl
from jax.experimental.pallas import tpu as pltpu
from jax.sharding import PartitionSpec as P

D = 2048
FF = 5632
RANK = 512
ROPE = 64
NOPE_W = 128
VAL_W = 128
NOPE_N = 64
VAL_N = 64
N_TP = 8
N_SP = 16
ROWS = 640
UNITS = FF // N_TP
FEATS = D // N_TP
EDGE = 16

theta = 10000.0
epsilon = 1e-06
LOG2E = 1.4426950408889634
SCALE_W = (NOPE_W + ROPE) ** -0.5 * LOG2E
SCALE_N = (NOPE_N + ROPE) ** -0.5 * LOG2E

MESH = pl.DeviceIdType.MESH
F32 = jnp.float32
BF16 = jnp.bfloat16

ORDER = (
    (0, 0), (1, 0), (3, 0), (2, 0), (0, 1), (0, 3), (3, 1), (3, 3),
    (1, 1), (1, 3), (0, 2), (2, 1), (2, 3), (1, 2), (3, 2), (2, 2),
)
SLOT = {offset: index for index, offset in enumerate(ORDER)}
PAIRS = len(ORDER) // 2
KEYS = 1280
CHUNK = 64
PLANE = 192
SCHEDULE = {
    "s0": "E3 E4", "m0": "E6 P1", "s1": "E5 X2", "m1": "E7 X3 P2", "s2": "E8", "m2": "E9 X4 P3", "s3": "E10", "m3": "X5 P4",
    "m4": "X6 P5", "m5": "X7 P6", "m6": "P7",
}
TAKEN = {
    "E3": ((0, 1), (0, 3)), "E4": ((2, 0),), "E5": ((1, 1), (1, 3)), "E6": ((3, 1), (3, 3)), "E7": ((2, 1), (2, 3)),
    "E8": ((0, 2),), "E9": ((1, 2), (3, 2)), "E10": ((2, 2),),
}
PLAN = {"s2": "U0", "s5": "U1", "heads": "U2 D0", "ended": "U3 D1", "joined": "U4 D2", "up": "D3", "conv": "D4"}
STEPS = (
    ((0, 0),),
    ((1, 0), (3, 0), (0, 1), (0, 3)),
    ((2, 0), (1, 1), (1, 3), (3, 1), (3, 3)),
    ((0, 2), (2, 1), (2, 3)),
    ((1, 2), (3, 2), (2, 2)),
)


class Place:
    def __init__(self):
        self.sp = lax.axis_index("sp")
        self.tp = lax.axis_index("tp")
        self.z, self.y = lax.div(self.sp, 4), lax.rem(self.sp, 4)
        self.x, self.c = lax.div(self.tp, 2), lax.rem(self.tp, 2)

    def along(self, first, second):
        z = lax.rem(self.z + first * (1 - self.c) + second * self.c, 4)
        y = lax.rem(self.y + first * self.c + second * (1 - self.c), 4)
        return z * 4 + y

    def device(self, first, second):
        return {"sp": self.along(first, second), "tp": self.tp}

    def feature(self, dx, other=0):
        core = self.c if not other else 1 - self.c
        return lax.rem(self.x + dx, 4) * 2 + core

    def peer(self, dx, other=0):
        return {"sp": self.sp, "tp": self.feature(dx, other)}


class Copies:
    def __init__(self):
        self.sent = []

    def start(self, build):
        def copy():
            src, dst, send, recv, device = build()
            return pltpu.make_async_remote_copy(
                src_ref=src, dst_ref=dst, send_sem=send, recv_sem=recv, device_id=device, device_id_type=MESH
            )

        copy().start()
        self.sent.append(copy)

    def arrived(self, dst, recv, device):
        pltpu.make_async_remote_copy(
            src_ref=dst, dst_ref=dst, send_sem=recv, recv_sem=recv, device_id=device, device_id_type=MESH
        ).wait_recv()

    def drain(self):
        for copy in self.sent:
            copy().wait_send()
        self.sent = []


def onward(offset):
    df, ds = offset
    moves = []
    if ds == 0:
        if df == 3:
            moves.append((1, 0, 0, (2, 0)))
        if df == 1:
            moves.append((3, 0, 1, (2, 0)))
        if df == 0:
            moves.append((1, 0, 0, (3, 0)))
            moves.append((3, 0, 1, (1, 0)))
            moves.append((1, 0, 1, (3, 0)))
            moves.append((3, 0, 0, (1, 0)))
        moves.append((0, 1, None, (df, 3)))
        moves.append((0, 3, None, (df, 1)))
    elif ds == 3:
        moves.append((0, 1, 0, (df, 2)))
    elif ds == 1:
        moves.append((0, 3, 1, (df, 2)))
    return moves


MOVES = [(offset, move) for offset in ORDER for move in onward(offset)]
SEND = {key: index for index, key in enumerate(MOVES)}
N_SEND = len(MOVES)


class Gather:
    def __init__(self, copies, place, view, send, recv):
        self.copies, self.place, self.view = copies, place, view
        self.send, self.recv = send, recv

    def forward(self, offset, only=lambda move: True):
        for move in filter(only, onward(offset)):
            for part in range(self.send.shape[0]):
                self.copies.start(lambda move=move, part=part: self._copy(offset, move, part))

    def _copy(self, offset, move, part):
        first, second, half, target = move
        return (
            self.view(offset, half, target)[part],
            self.landing(offset, target, half)[part],
            self.send.at[part, SEND[(offset, move)]],
            self.recv.at[part, SLOT[target] * 2 + (half or 0)],
            self.place.device(first, second),
        )

    def landing(self, offset, target, half):
        return self.view(target, half, target)

    def wait(self, offset, halves=None):
        if offset == (0, 0):
            return
        if halves is None:
            halves = (0, 1) if offset[1] in (0, 2) else (None,)
        for half in halves:
            for part, dst in enumerate(self.view(offset, half, offset)):
                self.copies.arrived(
                    dst, self.recv.at[part, SLOT[offset] * 2 + (half or 0)], self.place.device(0, 1)
                )


class GatherPlaced(Gather):
    def landing(self, offset, target, half):
        return self.view(offset, half, target)


class RingGather:
    def __init__(self, copies, place, view, send, recv):
        self.copies, self.place, self.view = copies, place, view
        self.send, self.recv = send, recv

    def _send(self, feature, half, index, arrival, device, parts=None):
        for part, ref in enumerate(self.view(feature, half)):
            if parts is not None and part not in parts:
                continue
            self.copies.start(
                lambda part=part, ref=ref: (ref, ref, self.send.at[part, index], self.recv.at[part, arrival], device)
            )

    def _wait(self, feature, half, arrival):
        for part, ref in enumerate(self.view(feature, half)):
            self.copies.arrived(ref, self.recv.at[part, arrival], self.place.peer(0, 1))

    def begin(self, parts=None):
        place = self.place
        me = place.feature(0)
        self._send(me, 0, 0, 0, place.peer(1), parts)
        self._send(me, 1, 1, 3, place.peer(3), parts)
        self._send(me, 1, 2, 1, place.peer(1), parts)
        self._send(me, 0, 3, 2, place.peer(3), parts)
        self._send(me, None, 4, 6, place.peer(0, 1), parts)

    def middle(self):
        place = self.place
        left, right = place.feature(3), place.feature(1)
        self._wait(left, 0, 0)
        self._send(left, 0, 5, 4, place.peer(1))
        self._wait(right, 1, 3)
        self._send(right, 1, 6, 5, place.peer(3))
        self._wait(left, 1, 1)
        self._send(left, None, 7, 7, place.peer(0, 1))
        self._wait(right, 0, 2)
        self._send(right, None, 8, 8, place.peer(0, 1))

    def end(self):
        place = self.place
        far = place.feature(2)
        self._wait(far, 0, 4)
        self._wait(far, 1, 5)
        self._send(far, None, 9, 9, place.peer(0, 1))
        self._wait(place.feature(0, 1), None, 6)
        self._wait(place.feature(3, 1), None, 7)
        self._wait(place.feature(1, 1), None, 8)
        self._wait(place.feature(2, 1), None, 9)


def half_rows(half, rows, start=0):
    if half is None:
        return pl.ds(start, rows)
    return pl.ds(start + half * (rows // 2), rows // 2)


def kernel(
    qw_hbm, qn_hbm, lat_hbm, rope_hbm, lgain_hbm, ew_hbm, en_hbm, res_hbm, ow_ref, on_ref, gain_ref, ug_ref, uv_ref, dn_ref,
    taps_hbm, inv_hbm, out_ref,
    latb, ropb, upf, dnf, kbuf, vbuf, sbuf, pbuf, mrow, acc, hw, hn, oww, ownr, own0, own1, gains, att, nrm, gx, vx, hid,
    part, send_a, recv_a, send_b, recv_b, send_c, recv_c,
    qt, qraw, qw_ref, qn_ref, lraw, rraw, lgain, ew_ref, en_ref, res_ref, taps_ref, inv_ref,
    ls, lr, xls, xlr, lps, lpr, us, ur, ds_, dr, hs, hr, as_, ar, xs, xr, es, er, rs, rr, local,
):
    place = Place()
    copies = Copies()
    c, tp, sp = place.c, place.tp, place.sp

    mine = pl.ds(pl.multiple_of(tp * FEATS, FEATS), FEATS)
    loads = [
        (lat_hbm, lraw), (rope_hbm, rraw), (lgain_hbm, lgain), (inv_hbm, inv_ref), (qw_hbm, qt), (qn_hbm, qraw),
        (ew_hbm, ew_ref), (en_hbm, en_ref), (ug_ref, upf.at[sp, 0:UNITS]), (uv_ref, upf.at[sp, UNITS : 2 * UNITS]),
        (dn_ref, dnf.at[sp]), (ow_ref.at[:, mine], oww.at[tp]), (on_ref.at[:, mine], ownr.at[tp]),
        (gain_ref, gains.at[tp]), (res_hbm, res_ref), (taps_hbm, taps_ref),
    ]

    def load(index):
        src, dst = loads[index]
        return pltpu.make_async_copy(src, dst, local.at[index])

    for index in range(len(loads)):
        load(index).start()

    barrier = pltpu.get_barrier_semaphore()
    talk = [place.device(f, s) for f, s in ((1, 0), (3, 0), (0, 1), (0, 3))]
    talk += [{"sp": sp, "tp": lax.rem(tp + d, N_TP)} for d in range(1, N_TP)]
    talk += [{"sp": lax.rem(sp + d, N_SP), "tp": tp} for d in (1, N_SP - 1)]
    for device in talk:
        pl.semaphore_signal(barrier, inc=1, device_id=device, device_id_type=MESH)

    for index in range(4):
        load(index).wait()
    for half in range(2):
        floats = lraw[half * 320 : half * 320 + 320, :].astype(F32)
        mean = jnp.sum(floats * floats, axis=1, keepdims=True) * (1.0 / RANK)
        latb[half, 0] = (floats * lax.rsqrt(mean + epsilon) * lgain[...]).astype(BF16)
    position = (lax.broadcasted_iota(jnp.int32, (32, ROWS), 1) + sp * ROWS).astype(F32)
    angles = position * inv_ref[:, 0:1]
    cosine, sine = jnp.cos(angles), jnp.sin(angles)

    def turn(floats):
        lower, upper = floats[0:32], floats[32:64]
        return [lower * cosine - upper * sine, lower * sine + upper * cosine]

    turned = turn(rraw[...].astype(F32))
    doubled = jnp.transpose(jnp.concatenate(turned + turned, axis=0))
    lane = lax.broadcasted_iota(jnp.int32, (160, 128), 1)
    for half in range(2):
        start = half * 320
        ropb[half, 0] = jnp.where(lane < 64, doubled[start : start + 160], doubled[start + 160 : start + 320]).astype(BF16)

    pl.semaphore_wait(barrier, len(talk))

    def lat_rows(half, target):
        if target[1] == 0:
            return half_rows(half, 320)
        start = lax.rem(place.x, 2) * (320 - PLANE)
        if half is None:
            return pl.ds(pl.multiple_of(start, 16), PLANE)
        return pl.ds(pl.multiple_of(start + half * (PLANE // 2), 16), PLANE // 2)

    def lat_view(offset, half, target):
        slot = SLOT[offset]
        return [latb.at[c, slot, lat_rows(half, target)], ropb.at[c, slot, half_rows(half, 160)]]

    def side_rows(slot, index, sent):
        parity = lax.rem(place.x + (0 if sent else 1), 2)
        start = parity * PLANE + index * (160 - PLANE // 2)
        return latb.at[c, slot, pl.ds(pl.multiple_of(start, 16), 160 - PLANE // 2)]

    lat_gather = Gather(copies, place, lat_view, ls, lr)

    def up_view(offset, half, target):
        return [upf.at[place.along(*offset), half_rows(half, 2 * UNITS)]]

    def dn_view(offset, half, target):
        return [dnf.at[place.along(*offset), half_rows(half, UNITS)]]

    up_gather = GatherPlaced(copies, place, up_view, us, ur)
    dn_gather = GatherPlaced(copies, place, dn_view, ds_, dr)

    lat_gather.forward((0, 0), lambda move: move[3][1] == 0)

    def exchange(d, start):
        to, source = lax.rem(tp + d, N_TP), lax.rem(tp + N_TP - d, N_TP)
        theirs = pl.ds(pl.multiple_of(to * FEATS, FEATS), FEATS)
        arrays = (
            (ow_ref.at[:, theirs], oww.at[tp], oww.at[source]),
            (on_ref.at[:, theirs], ownr.at[tp], ownr.at[source]),
            (gain_ref, gains.at[tp], gains.at[source]),
        )
        for index, (src, dst, landed) in enumerate(arrays):
            if start:
                copies.start(
                    lambda src=src, dst=dst, index=index: (
                        src, dst, xs.at[index, d], xr.at[index, d], {"sp": sp, "tp": to}
                    )
                )
            else:
                copies.arrived(landed, xr.at[index, d], {"sp": sp, "tp": to})

    for d in range(1, N_TP):
        exchange(d, True)

    for index in (4, 5):
        load(index).wait()
    blank = jnp.zeros((64, ROWS), F32)
    rope_part = [SCALE_W * piece for piece in turn(qt[128:192, :].astype(F32))]
    qw_ref[:, 0:128] = jnp.transpose(qt[0:128, :].astype(F32)).astype(BF16)
    qw_ref[:, 128:256] = jnp.transpose(jnp.concatenate([blank] + rope_part, axis=0)).astype(BF16)
    narrow_query = jnp.transpose(qraw[...].astype(F32))
    rope_part = [SCALE_N * piece for piece in turn(narrow_query[64:128])]
    qn_ref[...] = jnp.transpose(jnp.concatenate([narrow_query[0:64]] + rope_part, axis=0)).astype(BF16)
    for index in (6, 7):
        load(index).wait()

    mrow[...] = jnp.full_like(mrow, -1e30)
    acc[...] = jnp.zeros_like(acc)

    def partner_view(core, slot):
        return [latb.at[core, slot], ropb.at[core, slot]]

    def weights_at(point):
        for name in PLAN.get(point, "").split():
            gather, step = (up_gather, dn_gather)[name[0] == "D"], int(name[1])
            if step == 0:
                for index in (8, 9) if name[0] == "U" else (10,):
                    load(index).wait()
            for offset in STEPS[step]:
                gather.wait(offset)
                gather.forward(offset)

    def across(offset):
        slot = SLOT[offset]
        for index in range(2):
            copies.start(
                lambda index=index: (
                    partner_view(c, slot)[index], partner_view(c, slot)[index],
                    lps.at[index, slot], lpr.at[index, slot], place.peer(0, 1),
                )
            )

    def plane_arrival(offset):
        slot = SLOT[offset]
        lat_gather.wait(offset)
        lat_gather.forward(offset)
        if offset[1] == 0:
            across(offset)
            return
        for index, dx in enumerate((1, 3)):
            copies.start(
                lambda index=index, dx=dx: (
                    side_rows(slot, index, True), side_rows(slot, index, True),
                    xls.at[index, slot], xlr.at[index, slot], place.peer(dx),
                )
            )

    def side_arrival(offset):
        slot = SLOT[offset]
        for index in range(2):
            copies.arrived(side_rows(slot, index, False), xlr.at[index, slot], place.peer(1))
        across(offset)

    def partner_arrival(offset):
        slot = SLOT[offset]
        for index, ref in enumerate(partner_view(1 - c, slot)):
            copies.arrived(ref, lpr.at[index, slot], place.peer(0, 1))

    def take(point):
        for name in SCHEDULE.get(point, "").split():
            pair = int(name[1:])
            if name[0] == "E":
                for offset in TAKEN[name]:
                    plane_arrival(offset)
            else:
                for offset in ORDER[2 * pair : 2 * pair + 2]:
                    (side_arrival if name[0] == "X" else partner_arrival)(offset)
        weights_at(point)

    def expand(pair, side):
        lane = lax.broadcasted_iota(jnp.int32, (160, 128), 1)
        for u in range(4):
            block = latb[u % 2, 2 * pair + u // 2]
            rope = ropb[u % 2, 2 * pair + u // 2].astype(F32)
            wide = jnp.dot(block, ew_ref[...], preferred_element_type=F32)
            narrow = jnp.dot(block, en_ref[...], preferred_element_type=F32)
            rows = pl.ds(u * 320, 320)
            kbuf[side, rows, 0:128] = (wide[:, :128] * SCALE_W).astype(BF16)
            vbuf[side, rows, 0:128] = wide[:, 128:].astype(BF16)
            scaled = narrow * SCALE_N
            kbuf[side, pl.ds(u * 320, 160), 128:256] = jnp.where(
                lane < 64, scaled[:160], pltpu.roll(rope, 64, 1)
            ).astype(BF16)
            kbuf[side, pl.ds(u * 320 + 160, 160), 128:256] = jnp.where(lane < 64, scaled[160:], rope).astype(BF16)
            for row in (0, 160):
                vbuf[side, pl.ds(u * 320 + row, 160), 128:256] = jnp.where(lane < 64, 1.0, narrow[row : row + 160]).astype(
                    BF16
                )

    def score(group, side):
        q_ref, lanes = (qw_ref, slice(0, 256)) if group == 0 else (qn_ref, slice(128, 256))
        sbuf[group] = lax.dot_general(
            q_ref[...], kbuf[side, :, lanes], (((1,), (1,)), ((), ())), preferred_element_type=F32
        )

    def soften(group):
        for start in range(0, ROWS, CHUNK):
            rows = slice(start, start + CHUNK)
            kept = slice(group * ROWS + start, group * ROWS + start + CHUNK)
            scores = sbuf[group, rows, :]
            before = mrow[kept, :]
            top = jnp.maximum(before, jnp.max(scores, axis=1, keepdims=True))
            mrow[kept, :] = top
            pbuf[group, rows, :] = jnp.exp2(scores - top[:, 0:1]).astype(BF16)
            shrink = jnp.exp2(before - top)
            acc[kept, 0:128] = shrink * acc[kept, 0:128]
            if group == 0:
                acc[kept, 128:256] = shrink * acc[kept, 128:256]

    def gain_values(group, side):
        if group == 0:
            acc[0:ROWS, :] += jnp.dot(pbuf[0], vbuf[side], preferred_element_type=F32)
        else:
            acc[ROWS : 2 * ROWS, 0:128] += jnp.dot(pbuf[1], vbuf[side, :, 128:256], preferred_element_type=F32)

    pbuf[1] = jnp.zeros_like(pbuf[1])
    vbuf[1] = jnp.zeros_like(vbuf[1])
    for offset, half in (((3, 0), 0), ((1, 0), 1)):
        lat_gather.wait(offset, (half,))
        lat_gather.forward(offset, lambda move: move[3] == (2, 0))
    lat_gather.forward((0, 0), lambda move: move[3][1] != 0)
    for offset, half in (((1, 0), 0), ((3, 0), 1)):
        lat_gather.wait(offset, (half,))
        lat_gather.forward(offset, lambda move: move[3] != (2, 0))
        across(offset)
    partner_arrival((1, 0))
    expand(0, 0)
    score(0, 0)

    def attention_step(pair, carry):
        side = lax.rem(pair, 2)
        for k in range(PAIRS - 1):

            @pl.when(pair == k)
            def _():
                take(f"s{k}")

        score(1, side)
        gain_values(1, 1 - side)
        soften(0)
        for k in range(PAIRS - 1):

            @pl.when(pair == k)
            def _():
                take(f"m{k}")

        expand(pair + 1, 1 - side)
        gain_values(0, side)
        score(0, 1 - side)
        soften(1)
        return carry

    lax.fori_loop(0, PAIRS - 1, attention_step, 0)
    weights_at("last")
    last = (PAIRS - 1) % 2
    score(1, last)
    gain_values(1, 1 - last)
    soften(0)
    gain_values(0, last)
    hw[tp] = (acc[0:ROWS, 0:128] / acc[0:ROWS, 128:129]).astype(BF16)
    head_gather = RingGather(
        copies,
        place,
        lambda feature, half: [hw.at[feature, half_rows(half, 640)], hn.at[feature, half_rows(half, 320)]],
        hs,
        hr,
    )
    head_gather.begin((0,))
    soften(1)
    gain_values(1, last)

    low = acc[ROWS : ROWS + 320, 0:128] / acc[ROWS : ROWS + 320, 0:1]
    high = acc[ROWS + 320 : 2 * ROWS, 0:128] / acc[ROWS + 320 : 2 * ROWS, 0:1]
    lane = lax.broadcasted_iota(jnp.int32, (320, 128), 1)
    hn[tp] = jnp.where(lane < 64, pltpu.roll(low, 64, 1), high).astype(BF16)
    head_gather.begin((1,))

    weights_at("heads")

    for d in range(1, N_TP):
        exchange(d, False)
    for index in range(11, 16):
        load(index).wait()
    zero = jnp.zeros((64, FEATS), BF16)
    for j in range(N_TP):
        own0[pl.ds(j * 128, 64), :] = ownr[j]
        own0[pl.ds(j * 128 + 64, 64), :] = zero
        own1[pl.ds(j * 128, 64), :] = zero
        own1[pl.ds(j * 128 + 64, 64), :] = ownr[j]

    head_gather.middle()
    weights_at("middle")
    head_gather.end()
    weights_at("ended")

    wide_heads = jnp.concatenate([hw[j] for j in range(N_TP)], axis=1)
    narrow_heads = jnp.concatenate([hn[j] for j in range(N_TP)], axis=1)
    summed = jnp.dot(wide_heads, oww[...].reshape(N_TP * 128, FEATS), preferred_element_type=F32)
    top = jnp.dot(narrow_heads, own0[...], preferred_element_type=F32)
    bottom = jnp.dot(narrow_heads, own1[...], preferred_element_type=F32)
    att[tp, 0:320] = (res_ref[0:320, :].astype(F32) + summed[0:320] + top).astype(BF16)
    att[tp, 320:640] = (res_ref[320:640, :].astype(F32) + summed[320:640] + bottom).astype(BF16)

    att_gather = RingGather(
        copies, place, lambda feature, half: [att.at[feature, half_rows(half, 640)]], as_, ar
    )
    att_gather.begin()
    weights_at("begin")
    att_gather.middle()
    weights_at("joined")
    att_gather.end()
    weights_at("full")

    def norm_step(index, carry):
        rows = pl.ds(index * 64, 64)
        squares = jnp.zeros((64, FEATS), F32)
        for j in range(N_TP):
            piece = att[j, rows, :].astype(F32)
            squares = squares + piece * piece
        factor = lax.rsqrt(jnp.sum(squares, axis=1, keepdims=True) * (1.0 / D) + epsilon)
        for j in range(N_TP):
            nrm[rows, j * FEATS : (j + 1) * FEATS] = (
                att[j, rows, :].astype(F32) * factor * gains[j]
            ).astype(BF16)
        return carry

    lax.fori_loop(0, ROWS // 64, norm_step, 0)

    for base, dest in ((0, gx), (UNITS, vx)):
        for start in (0, 256, 512):
            stop = min(start + 256, UNITS)
            weights = jnp.concatenate([upf[o, base + start : base + stop, :] for o in range(N_SP)], axis=1)
            dest[EDGE : EDGE + ROWS, start:stop] = lax.dot_general(
                nrm[...], weights, (((1,), (1,)), ((), ())), preferred_element_type=F32
            ).astype(BF16)

    weights_at("up")
    following = {"sp": lax.rem(sp + 1, N_SP), "tp": tp}
    leading = {"sp": lax.rem(sp + N_SP - 1, N_SP), "tp": tp}
    edges = [
        (rows, landing, 2 * index + side, device)
        for side, (rows, landing, device) in enumerate(((ROWS, 0, following), (EDGE, ROWS + EDGE, leading)))
        for index in range(2)
    ]

    def edge(rows, landing, index, device):
        ref = (gx, vx)[index // 2]
        return ref.at[pl.ds(rows, EDGE)], ref.at[pl.ds(landing, EDGE)], es.at[index], er.at[index], device

    for entry in edges:
        copies.start(lambda entry=entry: edge(*entry))
    weights_at("edge")
    for rows, landing, index, device in edges:
        copies.arrived(edge(rows, landing, index, device)[1], er.at[index], device)

    def conv_step(index, carry):
        span = pl.ds(index * 128, 160)
        position = lax.broadcasted_iota(jnp.int32, (160, 1), 0) + index * 128 - EDGE
        outside = ((sp == 0) & (position < 0)) | ((sp == N_SP - 1) & (position >= ROWS))

        def smooth(ref, which, columns):
            wide = jnp.where(outside, 0.0, ref[span, columns].astype(F32))
            low = pltpu.roll(wide, 1, 0)[16:144]
            high = pltpu.roll(wide, 159, 0)[16:144]
            taps = [taps_ref[k, which : which + 1, columns] for k in range(3)]
            return taps[0] * low + taps[1] * wide[16:144] + taps[2] * high

        rows = pl.ds(index * 128, 128)
        for start in range(0, UNITS, 128):
            columns = slice(start, min(start + 128, UNITS))
            gate = smooth(gx, 0, columns)
            value = smooth(vx, 1, columns)
            hid[rows, columns] = (gate / (1.0 + jnp.exp(-gate)) * value).astype(BF16)
        return carry

    lax.fori_loop(0, 5, conv_step, 0)

    weights_at("conv")
    def down(feature):
        weights = jnp.concatenate([dnf[2 * feature], dnf[2 * feature + 1]], axis=1)
        return jnp.dot(hid[...], weights, preferred_element_type=F32)

    def down_pair(dx):
        send_a[dx] = down(place.feature(dx, 1)).astype(BF16)
        copies.start(lambda: (send_a.at[dx], recv_a.at[dx], rs.at[dx], rr.at[dx], place.peer(0, 1)))
        part[dx] = down(place.feature(dx))

    def pair_sum(dx):
        copies.arrived(recv_a.at[dx], rr.at[dx], place.peer(0, 1))
        return part[dx] + recv_a[dx].astype(F32)

    def send_half(side, index, dx):
        rows = pl.ds(320 * (index % 2), 320)
        copies.start(
            lambda: (send_c.at[side, rows], recv_c.at[side, rows], rs.at[6 + index], rr.at[6 + index], place.peer(dx))
        )

    down_pair(2)
    down_pair(1)
    far = pair_sum(2)
    send_b[0] = far[0:320].astype(BF16)
    copies.start(lambda: (send_b.at[0], recv_b.at[0], rs.at[4], rr.at[4], place.peer(1)))
    send_b[1] = far[320:640].astype(BF16)
    copies.start(lambda: (send_b.at[1], recv_b.at[1], rs.at[5], rr.at[5], place.peer(3)))
    down_pair(3)
    right = pair_sum(1)
    send_c[0, 320:640] = right[320:640].astype(BF16)
    send_half(0, 1, 1)
    part[1, 0:320] = right[0:320]
    down_pair(0)
    left = pair_sum(3)
    send_c[1, 0:320] = left[0:320].astype(BF16)
    send_half(1, 2, 3)
    copies.arrived(recv_b.at[0], rr.at[4], place.peer(1))
    send_c[0, 0:320] = (part[1, 0:320] + recv_b[0].astype(F32)).astype(BF16)
    send_half(0, 0, 1)
    copies.arrived(recv_b.at[1], rr.at[5], place.peer(3))
    send_c[1, 320:640] = (left[320:640] + recv_b[1].astype(F32)).astype(BF16)
    send_half(1, 3, 3)
    own_sum = pair_sum(0) + att[tp].astype(F32)
    for side, index in ((0, 1), (1, 2), (0, 0), (1, 3)):
        copies.arrived(recv_c.at[side, pl.ds(320 * (index % 2), 320)], rr.at[6 + index], place.peer(1))
    out_ref[...] = (own_sum + recv_c[0].astype(F32) + recv_c[1].astype(F32)).astype(BF16)
    copies.drain()


def per_device(
    residual, query_wide, query_narrow, latent, rope_key, latent_gain, expand_wide, expand_narrow,
    out_wide, out_narrow, norm_gain, up_gate, up_value, down_weight, conv_taps,
):
    inverse = np.power(np.float32(theta), -2.0 * np.arange(32, dtype=np.float32) / ROPE).astype(np.float32)
    inverse = jnp.asarray(np.broadcast_to(inverse[:, None], (32, 128)))
    vmem = pl.BlockSpec(memory_space=pltpu.VMEM)
    anywhere = pl.BlockSpec(memory_space=pl.ANY)
    dma = pltpu.SemaphoreType.DMA
    return pl.pallas_call(
        kernel,
        out_shape=jax.ShapeDtypeStruct((ROWS, FEATS), BF16),
        in_specs=[anywhere] * 16,
        out_specs=vmem,
        scratch_shapes=[
            pltpu.VMEM((2, 16, 320, RANK), BF16),
            pltpu.VMEM((2, 16, 160, 128), BF16),
            pltpu.VMEM((N_SP, 2 * UNITS, 128), BF16),
            pltpu.VMEM((N_SP, UNITS, 128), BF16),
            pltpu.VMEM((2, KEYS, 256), BF16),
            pltpu.VMEM((2, KEYS, 256), BF16),
            pltpu.VMEM((2, ROWS, KEYS), F32),
            pltpu.VMEM((2, ROWS, KEYS), BF16),
            pltpu.VMEM((2 * ROWS, 128), F32),
            pltpu.VMEM((2 * ROWS, 256), F32),
            pltpu.VMEM((N_TP, ROWS, 128), BF16),
            pltpu.VMEM((N_TP, ROWS // 2, 128), BF16),
            pltpu.VMEM((N_TP, 128, FEATS), BF16),
            pltpu.VMEM((N_TP, 64, FEATS), BF16),
            pltpu.VMEM((N_TP * 128, FEATS), BF16),
            pltpu.VMEM((N_TP * 128, FEATS), BF16),
            pltpu.VMEM((N_TP, 1, FEATS), F32),
            pltpu.VMEM((N_TP, ROWS, FEATS), BF16),
            pltpu.VMEM((ROWS, D), BF16),
            pltpu.VMEM((ROWS + 2 * EDGE, UNITS), BF16),
            pltpu.VMEM((ROWS + 2 * EDGE, UNITS), BF16),
            pltpu.VMEM((ROWS, UNITS), BF16),
            pltpu.VMEM((4, ROWS, FEATS), F32),
            pltpu.VMEM((4, ROWS, FEATS), BF16),
            pltpu.VMEM((4, ROWS, FEATS), BF16),
            pltpu.VMEM((2, ROWS // 2, FEATS), BF16),
            pltpu.VMEM((2, ROWS // 2, FEATS), BF16),
            pltpu.VMEM((2, ROWS, FEATS), BF16),
            pltpu.VMEM((2, ROWS, FEATS), BF16),
            pltpu.VMEM((NOPE_W + ROPE, ROWS), BF16),
            pltpu.VMEM((ROWS, 128), BF16),
            pltpu.VMEM((ROWS, 256), BF16),
            pltpu.VMEM((ROWS, 128), BF16),
            pltpu.VMEM((ROWS, RANK), BF16),
            pltpu.VMEM((ROPE, ROWS), BF16),
            pltpu.VMEM((1, RANK), F32),
            pltpu.VMEM((RANK, 256), BF16),
            pltpu.VMEM((RANK, 128), BF16),
            pltpu.VMEM((ROWS, FEATS), BF16),
            pltpu.VMEM((3, 2, UNITS), F32),
            pltpu.VMEM((32, 128), F32),
            dma((2, N_SEND)), dma((2, 32)), dma((2, 16)), dma((2, 16)), dma((2, 16)), dma((2, 16)),
            dma((1, N_SEND)), dma((1, 32)),
            dma((1, N_SEND)), dma((1, 32)),
            dma((2, 10)), dma((2, 10)),
            dma((1, 10)), dma((1, 10)),
            dma((3, 8)), dma((3, 8)),
            dma((4,)), dma((4,)),
            dma((10,)), dma((10,)),
            dma((16,)),
        ],
        compiler_params=pltpu.CompilerParams(
            collective_id=0, has_side_effects=True, vmem_limit_bytes=67043328
        ),
    )(
        query_wide.T, query_narrow, latent, rope_key.T, latent_gain.reshape(1, RANK), expand_wide, expand_narrow,
        residual, out_wide, out_narrow, norm_gain.reshape(1, FEATS), up_gate.T, up_value.T, down_weight.T, conv_taps, inverse,
    )


def solution(mesh):
    in_specs = (
        P("sp", "tp"), P("sp", "tp"), P("sp", "tp"), P("sp", None), P("sp", None), P(),
        P(None, "tp"), P(None, "tp"), P("tp", None), P("tp", None), P("tp"),
        P("sp", "tp"), P("sp", "tp"), P("sp", "tp"), P(None, None, "tp"),
    )
    return jax.shard_map(
        per_device, mesh=mesh, in_specs=in_specs, out_specs=P("sp", "tp"), check_vma=False
    )
```

```python
import jax
import jax.numpy as jnp
import numpy as np
from jax import lax
from jax.experimental import pallas as pl
from jax.experimental.pallas import tpu as pltpu
from jax.sharding import PartitionSpec as P

D = 2048
FF = 5632
RANK = 512
ROPE = 64
NOPE_W = 128
VAL_W = 128
NOPE_N = 64
VAL_N = 64
N_TP = 8
N_SP = 16
ROWS = 640
UNITS = FF // N_TP
FEATS = D // N_TP
EDGE = 16

theta = 10000.0
epsilon = 1e-06
LOG2E = 1.4426950408889634
SCALE_W = (NOPE_W + ROPE) ** -0.5 * LOG2E
SCALE_N = (NOPE_N + ROPE) ** -0.5 * LOG2E

MESH = pl.DeviceIdType.MESH
F32 = jnp.float32
BF16 = jnp.bfloat16

ORDER = (
    (0, 0), (1, 0), (3, 0), (2, 0), (0, 1), (0, 3), (3, 1), (3, 3),
    (1, 1), (1, 3), (0, 2), (2, 1), (2, 3), (1, 2), (3, 2), (2, 2),
)
SLOT = {offset: index for index, offset in enumerate(ORDER)}
PAIRS = len(ORDER) // 2
KEYS = 1280
CHUNK = 64
PLANE = 192
SCHEDULE = {
    "s0": "E3 E4", "m0": "E6 P1", "s1": "E5 X2", "m1": "E7 X3 P2", "s2": "E8", "m2": "E9 X4 P3", "s3": "E10", "m3": "X5 P4",
    "m4": "X6 P5", "m5": "X7 P6", "m6": "P7",
}
TAKEN = {
    "E3": ((0, 1), (0, 3)), "E4": ((2, 0),), "E5": ((1, 1), (1, 3)), "E6": ((3, 1), (3, 3)), "E7": ((2, 1), (2, 3)),
    "E8": ((0, 2),), "E9": ((1, 2), (3, 2)), "E10": ((2, 2),),
}
PLAN = {
    "s2": "U0", "s5": "U1", "heads": "U2 D0", "begin": "U3 D1", "joined": "U4 D2", "full": "D3", "edge": "D4",
}
STEPS = (
    ((0, 0),),
    ((1, 0), (3, 0), (0, 1), (0, 3)),
    ((2, 0), (1, 1), (1, 3), (3, 1), (3, 3)),
    ((0, 2), (2, 1), (2, 3)),
    ((1, 2), (3, 2), (2, 2)),
)


class Place:
    def __init__(self):
        self.sp = lax.axis_index("sp")
        self.tp = lax.axis_index("tp")
        self.z, self.y = lax.div(self.sp, 4), lax.rem(self.sp, 4)
        self.x, self.c = lax.div(self.tp, 2), lax.rem(self.tp, 2)

    def along(self, first, second):
        z = lax.rem(self.z + first * (1 - self.c) + second * self.c, 4)
        y = lax.rem(self.y + first * self.c + second * (1 - self.c), 4)
        return z * 4 + y

    def device(self, first, second):
        return {"sp": self.along(first, second), "tp": self.tp}

    def feature(self, dx, other=0):
        core = self.c if not other else 1 - self.c
        return lax.rem(self.x + dx, 4) * 2 + core

    def peer(self, dx, other=0):
        return {"sp": self.sp, "tp": self.feature(dx, other)}


class Copies:
    def __init__(self):
        self.sent = []

    def start(self, build):
        def copy():
            src, dst, send, recv, device = build()
            return pltpu.make_async_remote_copy(
                src_ref=src, dst_ref=dst, send_sem=send, recv_sem=recv, device_id=device, device_id_type=MESH
            )

        copy().start()
        self.sent.append(copy)

    def arrived(self, dst, recv, device):
        pltpu.make_async_remote_copy(
            src_ref=dst, dst_ref=dst, send_sem=recv, recv_sem=recv, device_id=device, device_id_type=MESH
        ).wait_recv()

    def drain(self):
        for copy in self.sent:
            copy().wait_send()
        self.sent = []


def onward(offset):
    df, ds = offset
    moves = []
    if ds == 0:
        if df == 3:
            moves.append((1, 0, 0, (2, 0)))
        if df == 1:
            moves.append((3, 0, 1, (2, 0)))
        if df == 0:
            moves.append((1, 0, 0, (3, 0)))
            moves.append((3, 0, 1, (1, 0)))
            moves.append((1, 0, 1, (3, 0)))
            moves.append((3, 0, 0, (1, 0)))
        moves.append((0, 1, None, (df, 3)))
        moves.append((0, 3, None, (df, 1)))
    elif ds == 3:
        moves.append((0, 1, 0, (df, 2)))
    elif ds == 1:
        moves.append((0, 3, 1, (df, 2)))
    return moves


MOVES = [(offset, move) for offset in ORDER for move in onward(offset)]
SEND = {key: index for index, key in enumerate(MOVES)}
N_SEND = len(MOVES)


class Gather:
    def __init__(self, copies, place, view, send, recv):
        self.copies, self.place, self.view = copies, place, view
        self.send, self.recv = send, recv

    def forward(self, offset, only=lambda move: True):
        for move in filter(only, onward(offset)):
            for part in range(self.send.shape[0]):
                self.copies.start(lambda move=move, part=part: self._copy(offset, move, part))

    def _copy(self, offset, move, part):
        first, second, half, target = move
        return (
            self.view(offset, half, target)[part],
            self.landing(offset, target, half)[part],
            self.send.at[part, SEND[(offset, move)]],
            self.recv.at[part, SLOT[target] * 2 + (half or 0)],
            self.place.device(first, second),
        )

    def landing(self, offset, target, half):
        return self.view(target, half, target)

    def wait(self, offset, halves=None):
        if offset == (0, 0):
            return
        if halves is None:
            halves = (0, 1) if offset[1] in (0, 2) else (None,)
        for half in halves:
            for part, dst in enumerate(self.view(offset, half, offset)):
                self.copies.arrived(
                    dst, self.recv.at[part, SLOT[offset] * 2 + (half or 0)], self.place.device(0, 1)
                )


class GatherPlaced(Gather):
    def landing(self, offset, target, half):
        return self.view(offset, half, target)


class RingGather:
    def __init__(self, copies, place, view, send, recv):
        self.copies, self.place, self.view = copies, place, view
        self.send, self.recv = send, recv

    def _send(self, feature, half, index, arrival, device, parts=None):
        for part, ref in enumerate(self.view(feature, half)):
            if parts is not None and part not in parts:
                continue
            self.copies.start(
                lambda part=part, ref=ref: (ref, ref, self.send.at[part, index], self.recv.at[part, arrival], device)
            )

    def _wait(self, feature, half, arrival):
        for part, ref in enumerate(self.view(feature, half)):
            self.copies.arrived(ref, self.recv.at[part, arrival], self.place.peer(0, 1))

    def begin(self, parts=None):
        place = self.place
        me = place.feature(0)
        self._send(me, 0, 0, 0, place.peer(1), parts)
        self._send(me, 1, 1, 3, place.peer(3), parts)
        self._send(me, 1, 2, 1, place.peer(1), parts)
        self._send(me, 0, 3, 2, place.peer(3), parts)
        self._send(me, None, 4, 6, place.peer(0, 1), parts)

    def middle(self):
        place = self.place
        left, right = place.feature(3), place.feature(1)
        self._wait(left, 0, 0)
        self._send(left, 0, 5, 4, place.peer(1))
        self._wait(right, 1, 3)
        self._send(right, 1, 6, 5, place.peer(3))
        self._wait(left, 1, 1)
        self._send(left, None, 7, 7, place.peer(0, 1))
        self._wait(right, 0, 2)
        self._send(right, None, 8, 8, place.peer(0, 1))

    def end(self):
        place = self.place
        far = place.feature(2)
        self._wait(far, 0, 4)
        self._wait(far, 1, 5)
        self._send(far, None, 9, 9, place.peer(0, 1))
        self._wait(place.feature(0, 1), None, 6)
        self._wait(place.feature(3, 1), None, 7)
        self._wait(place.feature(1, 1), None, 8)
        self._wait(place.feature(2, 1), None, 9)


def half_rows(half, rows, start=0):
    if half is None:
        return pl.ds(start, rows)
    return pl.ds(start + half * (rows // 2), rows // 2)


def kernel(
    qw_hbm, qn_hbm, lat_hbm, rope_hbm, lgain_hbm, ew_hbm, en_hbm, res_hbm, ow_ref, on_ref, gain_ref, ug_ref, uv_ref, dn_ref,
    taps_hbm, inv_hbm, out_ref,
    latb, ropb, upf, dnf, kbuf, vbuf, sbuf, pbuf, mrow, acc, hw, hn, oww, ownr, own0, own1, gains, att, nrm, gx, vx, hid,
    part, send_a, recv_a, send_b, recv_b, send_c, recv_c,
    qt, qraw, qw_ref, qn_ref, lraw, rraw, lgain, ew_ref, en_ref, res_ref, taps_ref, inv_ref,
    ls, lr, xls, xlr, lps, lpr, us, ur, ds_, dr, hs, hr, as_, ar, xs, xr, es, er, rs, rr, local,
):
    place = Place()
    copies = Copies()
    c, tp, sp = place.c, place.tp, place.sp

    mine = pl.ds(pl.multiple_of(tp * FEATS, FEATS), FEATS)
    loads = [
        (lat_hbm, lraw), (rope_hbm, rraw), (lgain_hbm, lgain), (inv_hbm, inv_ref), (qw_hbm, qt), (qn_hbm, qraw),
        (ew_hbm, ew_ref), (en_hbm, en_ref), (ug_ref, upf.at[sp, 0:UNITS]), (uv_ref, upf.at[sp, UNITS : 2 * UNITS]),
        (dn_ref, dnf.at[sp]), (ow_ref.at[:, mine], oww.at[tp]), (on_ref.at[:, mine], ownr.at[tp]),
        (gain_ref, gains.at[tp]), (res_hbm, res_ref), (taps_hbm, taps_ref),
    ]

    def load(index):
        src, dst = loads[index]
        return pltpu.make_async_copy(src, dst, local.at[index])

    for index in range(len(loads)):
        load(index).start()

    barrier = pltpu.get_barrier_semaphore()
    talk = [place.device(f, s) for f, s in ((1, 0), (3, 0), (0, 1), (0, 3))]
    talk += [{"sp": sp, "tp": lax.rem(tp + d, N_TP)} for d in range(1, N_TP)]
    talk += [{"sp": lax.rem(sp + d, N_SP), "tp": tp} for d in (1, N_SP - 1)]
    for device in talk:
        pl.semaphore_signal(barrier, inc=1, device_id=device, device_id_type=MESH)

    for index in range(4):
        load(index).wait()
    for half in range(2):
        floats = lraw[half * 320 : half * 320 + 320, :].astype(F32)
        mean = jnp.sum(floats * floats, axis=1, keepdims=True) * (1.0 / RANK)
        latb[half, 0] = (floats * lax.rsqrt(mean + epsilon) * lgain[...]).astype(BF16)
    position = (lax.broadcasted_iota(jnp.int32, (32, ROWS), 1) + sp * ROWS).astype(F32)
    angles = position * inv_ref[:, 0:1]
    cosine, sine = jnp.cos(angles), jnp.sin(angles)

    def turn(floats):
        lower, upper = floats[0:32], floats[32:64]
        return [lower * cosine - upper * sine, lower * sine + upper * cosine]

    turned = turn(rraw[...].astype(F32))
    doubled = jnp.transpose(jnp.concatenate(turned + turned, axis=0))
    lane = lax.broadcasted_iota(jnp.int32, (160, 128), 1)
    for half in range(2):
        start = half * 320
        ropb[half, 0] = jnp.where(lane < 64, doubled[start : start + 160], doubled[start + 160 : start + 320]).astype(BF16)

    pl.semaphore_wait(barrier, len(talk))

    def lat_rows(half, target):
        if target[1] == 0:
            return half_rows(half, 320)
        start = lax.rem(place.x, 2) * (320 - PLANE)
        if half is None:
            return pl.ds(pl.multiple_of(start, 16), PLANE)
        return pl.ds(pl.multiple_of(start + half * (PLANE // 2), 16), PLANE // 2)

    def lat_view(offset, half, target):
        slot = SLOT[offset]
        return [latb.at[c, slot, lat_rows(half, target)], ropb.at[c, slot, half_rows(half, 160)]]

    def side_rows(slot, index, sent):
        parity = lax.rem(place.x + (0 if sent else 1), 2)
        start = parity * PLANE + index * (160 - PLANE // 2)
        return latb.at[c, slot, pl.ds(pl.multiple_of(start, 16), 160 - PLANE // 2)]

    lat_gather = Gather(copies, place, lat_view, ls, lr)

    def up_view(offset, half, target):
        return [upf.at[place.along(*offset), half_rows(half, 2 * UNITS)]]

    def dn_view(offset, half, target):
        return [dnf.at[place.along(*offset), half_rows(half, UNITS)]]

    up_gather = GatherPlaced(copies, place, up_view, us, ur)
    dn_gather = GatherPlaced(copies, place, dn_view, ds_, dr)

    lat_gather.forward((0, 0), lambda move: move[3][1] == 0)

    def exchange(d, start):
        to, source = lax.rem(tp + d, N_TP), lax.rem(tp + N_TP - d, N_TP)
        theirs = pl.ds(pl.multiple_of(to * FEATS, FEATS), FEATS)
        arrays = (
            (ow_ref.at[:, theirs], oww.at[tp], oww.at[source]),
            (on_ref.at[:, theirs], ownr.at[tp], ownr.at[source]),
            (gain_ref, gains.at[tp], gains.at[source]),
        )
        for index, (src, dst, landed) in enumerate(arrays):
            if start:
                copies.start(
                    lambda src=src, dst=dst, index=index: (
                        src, dst, xs.at[index, d], xr.at[index, d], {"sp": sp, "tp": to}
                    )
                )
            else:
                copies.arrived(landed, xr.at[index, d], {"sp": sp, "tp": to})

    for d in range(1, N_TP):
        exchange(d, True)

    for index in (4, 5):
        load(index).wait()
    blank = jnp.zeros((64, ROWS), F32)
    rope_part = [SCALE_W * piece for piece in turn(qt[128:192, :].astype(F32))]
    qw_ref[:, 0:128] = jnp.transpose(qt[0:128, :].astype(F32)).astype(BF16)
    qw_ref[:, 128:256] = jnp.transpose(jnp.concatenate([blank] + rope_part, axis=0)).astype(BF16)
    narrow_query = jnp.transpose(qraw[...].astype(F32))
    rope_part = [SCALE_N * piece for piece in turn(narrow_query[64:128])]
    qn_ref[...] = jnp.transpose(jnp.concatenate([narrow_query[0:64]] + rope_part, axis=0)).astype(BF16)
    for index in (6, 7):
        load(index).wait()

    mrow[...] = jnp.full_like(mrow, -1e30)
    acc[...] = jnp.zeros_like(acc)

    def partner_view(core, slot):
        return [latb.at[core, slot], ropb.at[core, slot]]

    def weights_at(point):
        for name in PLAN.get(point, "").split():
            gather, step = (up_gather, dn_gather)[name[0] == "D"], int(name[1])
            if step == 0:
                for index in (8, 9) if name[0] == "U" else (10,):
                    load(index).wait()
            for offset in STEPS[step]:
                gather.wait(offset)
                gather.forward(offset)

    def across(offset):
        slot = SLOT[offset]
        for index in range(2):
            copies.start(
                lambda index=index: (
                    partner_view(c, slot)[index], partner_view(c, slot)[index],
                    lps.at[index, slot], lpr.at[index, slot], place.peer(0, 1),
                )
            )

    def plane_arrival(offset):
        slot = SLOT[offset]
        lat_gather.wait(offset)
        lat_gather.forward(offset)
        if offset[1] == 0:
            across(offset)
            return
        for index, dx in enumerate((1, 3)):
            copies.start(
                lambda index=index, dx=dx: (
                    side_rows(slot, index, True), side_rows(slot, index, True),
                    xls.at[index, slot], xlr.at[index, slot], place.peer(dx),
                )
            )

    def side_arrival(offset):
        slot = SLOT[offset]
        for index in range(2):
            copies.arrived(side_rows(slot, index, False), xlr.at[index, slot], place.peer(1))
        across(offset)

    def partner_arrival(offset):
        slot = SLOT[offset]
        for index, ref in enumerate(partner_view(1 - c, slot)):
            copies.arrived(ref, lpr.at[index, slot], place.peer(0, 1))

    def take(point):
        for name in SCHEDULE.get(point, "").split():
            pair = int(name[1:])
            if name[0] == "E":
                for offset in TAKEN[name]:
                    plane_arrival(offset)
            else:
                for offset in ORDER[2 * pair : 2 * pair + 2]:
                    (side_arrival if name[0] == "X" else partner_arrival)(offset)
        weights_at(point)

    def expand(pair, side):
        lane = lax.broadcasted_iota(jnp.int32, (160, 128), 1)
        for u in range(4):
            block = latb[u % 2, 2 * pair + u // 2]
            rope = ropb[u % 2, 2 * pair + u // 2].astype(F32)
            wide = jnp.dot(block, ew_ref[...], preferred_element_type=F32)
            narrow = jnp.dot(block, en_ref[...], preferred_element_type=F32)
            rows = pl.ds(u * 320, 320)
            kbuf[side, rows, 0:128] = (wide[:, :128] * SCALE_W).astype(BF16)
            vbuf[side, rows, 0:128] = wide[:, 128:].astype(BF16)
            scaled = narrow * SCALE_N
            kbuf[side, pl.ds(u * 320, 160), 128:256] = jnp.where(
                lane < 64, scaled[:160], pltpu.roll(rope, 64, 1)
            ).astype(BF16)
            kbuf[side, pl.ds(u * 320 + 160, 160), 128:256] = jnp.where(lane < 64, scaled[160:], rope).astype(BF16)
            for row in (0, 160):
                vbuf[side, pl.ds(u * 320 + row, 160), 128:256] = jnp.where(lane < 64, 1.0, narrow[row : row + 160]).astype(
                    BF16
                )

    def score(group, side):
        q_ref, lanes = (qw_ref, slice(0, 256)) if group == 0 else (qn_ref, slice(128, 256))
        sbuf[group] = lax.dot_general(
            q_ref[...], kbuf[side, :, lanes], (((1,), (1,)), ((), ())), preferred_element_type=F32
        )

    def soften(group):
        for start in range(0, ROWS, CHUNK):
            rows = slice(start, start + CHUNK)
            kept = slice(group * ROWS + start, group * ROWS + start + CHUNK)
            scores = sbuf[group, rows, :]
            before = mrow[kept, :]
            top = jnp.maximum(before, jnp.max(scores, axis=1, keepdims=True))
            mrow[kept, :] = top
            pbuf[group, rows, :] = jnp.exp2(scores - top[:, 0:1]).astype(BF16)
            shrink = jnp.exp2(before - top)
            acc[kept, 0:128] = shrink * acc[kept, 0:128]
            if group == 0:
                acc[kept, 128:256] = shrink * acc[kept, 128:256]

    def gain_values(group, side):
        if group == 0:
            acc[0:ROWS, :] += jnp.dot(pbuf[0], vbuf[side], preferred_element_type=F32)
        else:
            acc[ROWS : 2 * ROWS, 0:128] += jnp.dot(pbuf[1], vbuf[side, :, 128:256], preferred_element_type=F32)

    pbuf[1] = jnp.zeros_like(pbuf[1])
    vbuf[1] = jnp.zeros_like(vbuf[1])
    for offset, half in (((3, 0), 0), ((1, 0), 1)):
        lat_gather.wait(offset, (half,))
        lat_gather.forward(offset, lambda move: move[3] == (2, 0))
    lat_gather.forward((0, 0), lambda move: move[3][1] != 0)
    for offset, half in (((1, 0), 0), ((3, 0), 1)):
        lat_gather.wait(offset, (half,))
        lat_gather.forward(offset, lambda move: move[3] != (2, 0))
        across(offset)
    partner_arrival((1, 0))
    expand(0, 0)
    score(0, 0)

    def attention_step(pair, carry):
        side = lax.rem(pair, 2)
        for k in range(PAIRS - 1):

            @pl.when(pair == k)
            def _():
                take(f"s{k}")

        score(1, side)
        gain_values(1, 1 - side)
        soften(0)
        for k in range(PAIRS - 1):

            @pl.when(pair == k)
            def _():
                take(f"m{k}")

        expand(pair + 1, 1 - side)
        gain_values(0, side)
        score(0, 1 - side)
        soften(1)
        return carry

    lax.fori_loop(0, PAIRS - 1, attention_step, 0)
    weights_at("last")
    last = (PAIRS - 1) % 2
    score(1, last)
    gain_values(1, 1 - last)
    soften(0)
    gain_values(0, last)
    hw[tp] = (acc[0:ROWS, 0:128] / acc[0:ROWS, 128:129]).astype(BF16)
    head_gather = RingGather(
        copies,
        place,
        lambda feature, half: [hw.at[feature, half_rows(half, 640)], hn.at[feature, half_rows(half, 320)]],
        hs,
        hr,
    )
    head_gather.begin((0,))
    soften(1)
    gain_values(1, last)

    low = acc[ROWS : ROWS + 320, 0:128] / acc[ROWS : ROWS + 320, 0:1]
    high = acc[ROWS + 320 : 2 * ROWS, 0:128] / acc[ROWS + 320 : 2 * ROWS, 0:1]
    lane = lax.broadcasted_iota(jnp.int32, (320, 128), 1)
    hn[tp] = jnp.where(lane < 64, pltpu.roll(low, 64, 1), high).astype(BF16)
    head_gather.begin((1,))

    weights_at("heads")

    for d in range(1, N_TP):
        exchange(d, False)
    for index in range(11, 16):
        load(index).wait()
    zero = jnp.zeros((64, FEATS), BF16)
    for j in range(N_TP):
        own0[pl.ds(j * 128, 64), :] = ownr[j]
        own0[pl.ds(j * 128 + 64, 64), :] = zero
        own1[pl.ds(j * 128, 64), :] = zero
        own1[pl.ds(j * 128 + 64, 64), :] = ownr[j]

    head_gather.middle()
    weights_at("middle")
    head_gather.end()
    weights_at("ended")

    wide_heads = jnp.concatenate([hw[j] for j in range(N_TP)], axis=1)
    narrow_heads = jnp.concatenate([hn[j] for j in range(N_TP)], axis=1)
    summed = jnp.dot(wide_heads, oww[...].reshape(N_TP * 128, FEATS), preferred_element_type=F32)
    top = jnp.dot(narrow_heads, own0[...], preferred_element_type=F32)
    bottom = jnp.dot(narrow_heads, own1[...], preferred_element_type=F32)
    att[tp, 0:320] = (res_ref[0:320, :].astype(F32) + summed[0:320] + top).astype(BF16)
    att[tp, 320:640] = (res_ref[320:640, :].astype(F32) + summed[320:640] + bottom).astype(BF16)

    att_gather = RingGather(
        copies, place, lambda feature, half: [att.at[feature, half_rows(half, 640)]], as_, ar
    )
    att_gather.begin()
    weights_at("begin")
    att_gather.middle()
    weights_at("joined")
    att_gather.end()
    weights_at("full")

    def norm_step(index, carry):
        rows = pl.ds(index * 64, 64)
        squares = jnp.zeros((64, FEATS), F32)
        for j in range(N_TP):
            piece = att[j, rows, :].astype(F32)
            squares = squares + piece * piece
        factor = lax.rsqrt(jnp.sum(squares, axis=1, keepdims=True) * (1.0 / D) + epsilon)
        for j in range(N_TP):
            nrm[rows, j * FEATS : (j + 1) * FEATS] = (
                att[j, rows, :].astype(F32) * factor * gains[j]
            ).astype(BF16)
        return carry

    lax.fori_loop(0, ROWS // 64, norm_step, 0)

    for base, dest in ((0, gx), (UNITS, vx)):
        for start in (0, 256, 512):
            stop = min(start + 256, UNITS)
            weights = jnp.concatenate([upf[o, base + start : base + stop, :] for o in range(N_SP)], axis=1)
            dest[EDGE : EDGE + ROWS, start:stop] = lax.dot_general(
                nrm[...], weights, (((1,), (1,)), ((), ())), preferred_element_type=F32
            ).astype(BF16)

    weights_at("up")
    following = {"sp": lax.rem(sp + 1, N_SP), "tp": tp}
    leading = {"sp": lax.rem(sp + N_SP - 1, N_SP), "tp": tp}
    edges = [
        (rows, landing, 2 * index + side, device)
        for side, (rows, landing, device) in enumerate(((ROWS, 0, following), (EDGE, ROWS + EDGE, leading)))
        for index in range(2)
    ]

    def edge(rows, landing, index, device):
        ref = (gx, vx)[index // 2]
        return ref.at[pl.ds(rows, EDGE)], ref.at[pl.ds(landing, EDGE)], es.at[index], er.at[index], device

    for entry in edges:
        copies.start(lambda entry=entry: edge(*entry))
    weights_at("edge")

    def conv_step(index, place_of):
        span = pl.ds(index * 128, 160)
        position = lax.broadcasted_iota(jnp.int32, (160, 1), 0) + index * 128 - EDGE
        outside = ((sp == 0) & (position < 0)) | ((sp == N_SP - 1) & (position >= ROWS))

        def smooth(ref, which, columns):
            wide = jnp.where(outside, 0.0, ref[span, columns].astype(F32))
            low = pltpu.roll(wide, 1, 0)[16:144]
            high = pltpu.roll(wide, 159, 0)[16:144]
            taps = [taps_ref[k, which : which + 1, columns] for k in range(3)]
            return taps[0] * low + taps[1] * wide[16:144] + taps[2] * high

        rows = pl.ds(place_of * 128, 128)
        for start in range(0, UNITS, 128):
            columns = slice(start, min(start + 128, UNITS))
            gate = smooth(gx, 0, columns)
            value = smooth(vx, 1, columns)
            hid[rows, columns] = (gate / (1.0 + jnp.exp(-gate)) * value).astype(BF16)

    def inner_step(index, carry):
        conv_step(index, index - 1)
        return carry

    lax.fori_loop(1, 4, inner_step, 0)

    def down(feature, rows):
        weights = jnp.concatenate([dnf[2 * feature], dnf[2 * feature + 1]], axis=1)
        return jnp.dot(hid[rows, :], weights, preferred_element_type=F32)

    class Reduce:
        def __init__(self, start, count, first):
            self.rows = slice(start, start + count)
            self.halves = (slice(start, start + count // 2), slice(start + count // 2, start + count))
            self.first = first

        def move(self, ref, other, index, device):
            index += self.first
            copies.start(lambda: (ref(), other(), rs.at[index], rr.at[index], device()))

        def landed(self, ref, index):
            copies.arrived(ref, rr.at[index + self.first], place.peer(1))

        def down_pair(self, dx):
            rows = self.rows
            send_a[dx, rows] = down(place.feature(dx, 1), rows).astype(BF16)
            self.move(lambda: send_a.at[dx, rows], lambda: recv_a.at[dx, rows], dx, lambda: place.peer(0, 1))
            part[dx, rows] = down(place.feature(dx), rows)

        def pair_sum(self, dx):
            self.landed(recv_a.at[dx, self.rows], dx)
            return part[dx, self.rows] + recv_a[dx, self.rows].astype(F32)

        def far(self):
            total = self.pair_sum(2).astype(BF16)
            for side, rows in enumerate(self.halves):
                send_b[rows] = total[rows.start - self.rows.start : rows.stop - self.rows.start]
                self.move(
                    lambda rows=rows: send_b.at[rows], lambda rows=rows: recv_b.at[rows], 4 + side,
                    lambda side=side: place.peer((1, 3)[side]),
                )

        def near(self, side):
            total = self.pair_sum((1, 3)[side])
            part[(1, 3)[side], self.rows] = total
            rows = self.halves[1 - side]
            send_c[side, rows] = total[rows.start - self.rows.start : rows.stop - self.rows.start].astype(BF16)
            self.send(side, rows, 6 + side)

        def send(self, side, rows, index):
            self.move(
                lambda: send_c.at[side, rows], lambda: recv_c.at[side, rows], index, lambda: place.peer((1, 3)[side])
            )

        def join(self):
            for side, rows in enumerate(self.halves):
                self.landed(recv_b.at[rows], 4 + side)
                send_c[side, rows] = (part[(1, 3)[side], rows] + recv_b[rows].astype(F32)).astype(BF16)
                self.send(side, rows, 8 + side)

        def result(self):
            total = self.pair_sum(0)
            for side in range(2):
                self.landed(recv_c.at[side, self.halves[1 - side]], 6 + side)
                self.landed(recv_c.at[side, self.halves[side]], 8 + side)
            return total + recv_c[0, self.rows].astype(F32) + recv_c[1, self.rows].astype(F32)

    first, second = Reduce(0, 384, 0), Reduce(384, 256, 10)
    first.down_pair(2)
    first.down_pair(1)
    first.far()
    first.down_pair(3)
    first.near(0)
    first.down_pair(0)
    first.near(1)
    for rows, landing, index, device in edges:
        copies.arrived(edge(rows, landing, index, device)[1], er.at[index], device)
    conv_step(0, 3)
    conv_step(4, 4)
    second.down_pair(2)
    second.down_pair(1)
    second.far()
    second.down_pair(3)
    second.near(0)
    first.join()
    second.down_pair(0)
    second.near(1)
    second.join()
    out_ref[128:512, :] = (att[tp, 128:512].astype(F32) + first.result()).astype(BF16)
    rest = second.result()
    out_ref[0:128, :] = (att[tp, 0:128].astype(F32) + rest[0:128]).astype(BF16)
    out_ref[512:640, :] = (att[tp, 512:640].astype(F32) + rest[128:256]).astype(BF16)
    copies.drain()


def per_device(
    residual, query_wide, query_narrow, latent, rope_key, latent_gain, expand_wide, expand_narrow,
    out_wide, out_narrow, norm_gain, up_gate, up_value, down_weight, conv_taps,
):
    inverse = np.power(np.float32(theta), -2.0 * np.arange(32, dtype=np.float32) / ROPE).astype(np.float32)
    inverse = jnp.asarray(np.broadcast_to(inverse[:, None], (32, 128)))
    vmem = pl.BlockSpec(memory_space=pltpu.VMEM)
    anywhere = pl.BlockSpec(memory_space=pl.ANY)
    dma = pltpu.SemaphoreType.DMA
    return pl.pallas_call(
        kernel,
        out_shape=jax.ShapeDtypeStruct((ROWS, FEATS), BF16),
        in_specs=[anywhere] * 16,
        out_specs=vmem,
        scratch_shapes=[
            pltpu.VMEM((2, 16, 320, RANK), BF16),
            pltpu.VMEM((2, 16, 160, 128), BF16),
            pltpu.VMEM((N_SP, 2 * UNITS, 128), BF16),
            pltpu.VMEM((N_SP, UNITS, 128), BF16),
            pltpu.VMEM((2, KEYS, 256), BF16),
            pltpu.VMEM((2, KEYS, 256), BF16),
            pltpu.VMEM((2, ROWS, KEYS), F32),
            pltpu.VMEM((2, ROWS, KEYS), BF16),
            pltpu.VMEM((2 * ROWS, 128), F32),
            pltpu.VMEM((2 * ROWS, 256), F32),
            pltpu.VMEM((N_TP, ROWS, 128), BF16),
            pltpu.VMEM((N_TP, ROWS // 2, 128), BF16),
            pltpu.VMEM((N_TP, 128, FEATS), BF16),
            pltpu.VMEM((N_TP, 64, FEATS), BF16),
            pltpu.VMEM((N_TP * 128, FEATS), BF16),
            pltpu.VMEM((N_TP * 128, FEATS), BF16),
            pltpu.VMEM((N_TP, 1, FEATS), F32),
            pltpu.VMEM((N_TP, ROWS, FEATS), BF16),
            pltpu.VMEM((ROWS, D), BF16),
            pltpu.VMEM((ROWS + 2 * EDGE, UNITS), BF16),
            pltpu.VMEM((ROWS + 2 * EDGE, UNITS), BF16),
            pltpu.VMEM((ROWS, UNITS), BF16),
            pltpu.VMEM((4, ROWS, FEATS), F32),
            pltpu.VMEM((4, ROWS, FEATS), BF16),
            pltpu.VMEM((4, ROWS, FEATS), BF16),
            pltpu.VMEM((ROWS, FEATS), BF16),
            pltpu.VMEM((ROWS, FEATS), BF16),
            pltpu.VMEM((2, ROWS, FEATS), BF16),
            pltpu.VMEM((2, ROWS, FEATS), BF16),
            pltpu.VMEM((NOPE_W + ROPE, ROWS), BF16),
            pltpu.VMEM((ROWS, 128), BF16),
            pltpu.VMEM((ROWS, 256), BF16),
            pltpu.VMEM((ROWS, 128), BF16),
            pltpu.VMEM((ROWS, RANK), BF16),
            pltpu.VMEM((ROPE, ROWS), BF16),
            pltpu.VMEM((1, RANK), F32),
            pltpu.VMEM((RANK, 256), BF16),
            pltpu.VMEM((RANK, 128), BF16),
            pltpu.VMEM((ROWS, FEATS), BF16),
            pltpu.VMEM((3, 2, UNITS), F32),
            pltpu.VMEM((32, 128), F32),
            dma((2, N_SEND)), dma((2, 32)), dma((2, 16)), dma((2, 16)), dma((2, 16)), dma((2, 16)),
            dma((1, N_SEND)), dma((1, 32)),
            dma((1, N_SEND)), dma((1, 32)),
            dma((2, 10)), dma((2, 10)),
            dma((1, 10)), dma((1, 10)),
            dma((3, 8)), dma((3, 8)),
            dma((4,)), dma((4,)),
            dma((20,)), dma((20,)),
            dma((16,)),
        ],
        compiler_params=pltpu.CompilerParams(
            collective_id=0, has_side_effects=True, vmem_limit_bytes=67043328
        ),
    )(
        query_wide.T, query_narrow, latent, rope_key.T, latent_gain.reshape(1, RANK), expand_wide, expand_narrow,
        residual, out_wide, out_narrow, norm_gain.reshape(1, FEATS), up_gate.T, up_value.T, down_weight.T, conv_taps, inverse,
    )


def solution(mesh):
    in_specs = (
        P("sp", "tp"), P("sp", "tp"), P("sp", "tp"), P("sp", None), P("sp", None), P(),
        P(None, "tp"), P(None, "tp"), P("tp", None), P("tp", None), P("tp"),
        P("sp", "tp"), P("sp", "tp"), P("sp", "tp"), P(None, None, "tp"),
    )
    return jax.shard_map(
        per_device, mesh=mesh, in_specs=in_specs, out_specs=P("sp", "tp"), check_vma=False
    )
```

```python
import jax
import jax.numpy as jnp
import numpy as np
from jax import lax
from jax.experimental import pallas as pl
from jax.experimental.pallas import tpu as pltpu
from jax.sharding import PartitionSpec as P

D = 2048
FF = 5632
RANK = 512
ROPE = 64
NOPE_W = 128
VAL_W = 128
NOPE_N = 64
VAL_N = 64
N_TP = 8
N_SP = 16
ROWS = 640
UNITS = FF // N_TP
FEATS = D // N_TP
EDGE = 16

theta = 10000.0
epsilon = 1e-06
LOG2E = 1.4426950408889634
SCALE_W = (NOPE_W + ROPE) ** -0.5 * LOG2E
SCALE_N = (NOPE_N + ROPE) ** -0.5 * LOG2E

MESH = pl.DeviceIdType.MESH
F32 = jnp.float32
BF16 = jnp.bfloat16

ORDER = (
    (0, 0), (1, 0), (3, 0), (2, 0), (0, 1), (0, 3), (3, 1), (3, 3),
    (1, 1), (1, 3), (0, 2), (2, 1), (2, 3), (1, 2), (3, 2), (2, 2),
)
SLOT = {offset: index for index, offset in enumerate(ORDER)}
PAIRS = len(ORDER) // 2
KEYS = 1280
CHUNK = 64
PLANE = 192
SCHEDULE = {
    "s0": "E3 E4", "m0": "E6 P1", "s1": "E5 X2", "m1": "E7 X3 P2", "s2": "E8", "m2": "E9 X4 P3", "s3": "E10", "m3": "X5 P4",
    "m4": "X6 P5", "m5": "X7 P6", "m6": "P7",
}
TAKEN = {
    "E3": ((0, 1), (0, 3)), "E4": ((2, 0),), "E5": ((1, 1), (1, 3)), "E6": ((3, 1), (3, 3)), "E7": ((2, 1), (2, 3)),
    "E8": ((0, 2),), "E9": ((1, 2), (3, 2)), "E10": ((2, 2),),
}
PLAN = {
    "s2": "U0", "s5": "U1", "heads": "U2 D0", "begin": "U3 D1", "joined": "U4 D2", "full": "D3", "edge": "D4",
}
STEPS = (
    ((0, 0),),
    ((1, 0), (3, 0), (0, 1), (0, 3)),
    ((2, 0), (1, 1), (1, 3), (3, 1), (3, 3)),
    ((0, 2), (2, 1), (2, 3)),
    ((1, 2), (3, 2), (2, 2)),
)


class Place:
    def __init__(self):
        self.sp = lax.axis_index("sp")
        self.tp = lax.axis_index("tp")
        self.z, self.y = lax.div(self.sp, 4), lax.rem(self.sp, 4)
        self.x, self.c = lax.div(self.tp, 2), lax.rem(self.tp, 2)

    def along(self, first, second):
        z = lax.rem(self.z + first * (1 - self.c) + second * self.c, 4)
        y = lax.rem(self.y + first * self.c + second * (1 - self.c), 4)
        return z * 4 + y

    def device(self, first, second):
        return {"sp": self.along(first, second), "tp": self.tp}

    def feature(self, dx, other=0):
        core = self.c if not other else 1 - self.c
        return lax.rem(self.x + dx, 4) * 2 + core

    def peer(self, dx, other=0):
        return {"sp": self.sp, "tp": self.feature(dx, other)}


class Copies:
    def __init__(self):
        self.sent = []

    def start(self, build):
        def copy():
            src, dst, send, recv, device = build()
            return pltpu.make_async_remote_copy(
                src_ref=src, dst_ref=dst, send_sem=send, recv_sem=recv, device_id=device, device_id_type=MESH
            )

        copy().start()
        self.sent.append(copy)

    def arrived(self, dst, recv, device):
        pltpu.make_async_remote_copy(
            src_ref=dst, dst_ref=dst, send_sem=recv, recv_sem=recv, device_id=device, device_id_type=MESH
        ).wait_recv()

    def drain(self):
        for copy in self.sent:
            copy().wait_send()
        self.sent = []


def onward(offset):
    df, ds = offset
    moves = []
    if ds == 0:
        if df == 3:
            moves.append((1, 0, 0, (2, 0)))
        if df == 1:
            moves.append((3, 0, 1, (2, 0)))
        if df == 0:
            moves.append((1, 0, 0, (3, 0)))
            moves.append((3, 0, 1, (1, 0)))
            moves.append((1, 0, 1, (3, 0)))
            moves.append((3, 0, 0, (1, 0)))
        moves.append((0, 1, None, (df, 3)))
        moves.append((0, 3, None, (df, 1)))
    elif ds == 3:
        moves.append((0, 1, 0, (df, 2)))
    elif ds == 1:
        moves.append((0, 3, 1, (df, 2)))
    return moves


MOVES = [(offset, move) for offset in ORDER for move in onward(offset)]
SEND = {key: index for index, key in enumerate(MOVES)}
N_SEND = len(MOVES)


class Gather:
    def __init__(self, copies, place, view, send, recv):
        self.copies, self.place, self.view = copies, place, view
        self.send, self.recv = send, recv

    def forward(self, offset, only=lambda move: True):
        for move in filter(only, onward(offset)):
            for part in range(self.send.shape[0]):
                self.copies.start(lambda move=move, part=part: self._copy(offset, move, part))

    def _copy(self, offset, move, part):
        first, second, half, target = move
        return (
            self.view(offset, half, target)[part],
            self.landing(offset, target, half)[part],
            self.send.at[part, SEND[(offset, move)]],
            self.recv.at[part, SLOT[target] * 2 + (half or 0)],
            self.place.device(first, second),
        )

    def landing(self, offset, target, half):
        return self.view(target, half, target)

    def wait(self, offset, halves=None):
        if offset == (0, 0):
            return
        if halves is None:
            halves = (0, 1) if offset[1] in (0, 2) else (None,)
        for half in halves:
            for part, dst in enumerate(self.view(offset, half, offset)):
                self.copies.arrived(
                    dst, self.recv.at[part, SLOT[offset] * 2 + (half or 0)], self.place.device(0, 1)
                )


class GatherPlaced(Gather):
    def landing(self, offset, target, half):
        return self.view(offset, half, target)


class RingGather:
    def __init__(self, copies, place, view, send, recv):
        self.copies, self.place, self.view = copies, place, view
        self.send, self.recv = send, recv

    def _send(self, feature, half, index, arrival, device, parts=None):
        for part, ref in enumerate(self.view(feature, half)):
            if parts is not None and part not in parts:
                continue
            self.copies.start(
                lambda part=part, ref=ref: (ref, ref, self.send.at[part, index], self.recv.at[part, arrival], device)
            )

    def _wait(self, feature, half, arrival):
        for part, ref in enumerate(self.view(feature, half)):
            self.copies.arrived(ref, self.recv.at[part, arrival], self.place.peer(0, 1))

    def begin(self, parts=None):
        place = self.place
        me = place.feature(0)
        self._send(me, 0, 0, 0, place.peer(1), parts)
        self._send(me, 1, 1, 3, place.peer(3), parts)
        self._send(me, 1, 2, 1, place.peer(1), parts)
        self._send(me, 0, 3, 2, place.peer(3), parts)
        self._send(me, None, 4, 6, place.peer(0, 1), parts)

    def middle(self):
        place = self.place
        left, right = place.feature(3), place.feature(1)
        self._wait(left, 0, 0)
        self._send(left, 0, 5, 4, place.peer(1))
        self._wait(right, 1, 3)
        self._send(right, 1, 6, 5, place.peer(3))
        self._wait(left, 1, 1)
        self._send(left, None, 7, 7, place.peer(0, 1))
        self._wait(right, 0, 2)
        self._send(right, None, 8, 8, place.peer(0, 1))

    def end(self):
        place = self.place
        far = place.feature(2)
        self._wait(far, 0, 4)
        self._wait(far, 1, 5)
        self._send(far, None, 9, 9, place.peer(0, 1))
        self._wait(place.feature(0, 1), None, 6)
        self._wait(place.feature(3, 1), None, 7)
        self._wait(place.feature(1, 1), None, 8)
        self._wait(place.feature(2, 1), None, 9)


def half_rows(half, rows, start=0):
    if half is None:
        return pl.ds(start, rows)
    return pl.ds(start + half * (rows // 2), rows // 2)


def kernel(
    qw_hbm, qn_hbm, lat_hbm, rope_hbm, lgain_hbm, ew_hbm, en_hbm, res_hbm, ow_ref, on_ref, gain_ref, ug_ref, uv_ref, dn_ref,
    taps_hbm, inv_hbm, out_ref,
    latb, ropb, upf, dnf, kbuf, vbuf, sbuf, pbuf, mrow, acc, hw, hn, oww, ownr, own0, own1, gains, att, nrm, gx, vx, hid,
    part, send_a, recv_a, send_b, recv_b, send_c, recv_c,
    qt, qraw, qw_ref, qn_ref, lraw, rraw, lgain, ew_ref, en_ref, res_ref, taps_ref, inv_ref,
    ls, lr, xls, xlr, lps, lpr, us, ur, ds_, dr, hs, hr, as_, ar, xs, xr, es, er, rs, rr, local,
):
    place = Place()
    copies = Copies()
    c, tp, sp = place.c, place.tp, place.sp

    mine = pl.ds(pl.multiple_of(tp * FEATS, FEATS), FEATS)
    loads = [
        (lat_hbm, lraw), (rope_hbm, rraw), (lgain_hbm, lgain), (inv_hbm, inv_ref), (qw_hbm, qt), (qn_hbm, qraw),
        (ew_hbm, ew_ref), (en_hbm, en_ref), (ug_ref, upf.at[sp, 0:UNITS]), (uv_ref, upf.at[sp, UNITS : 2 * UNITS]),
        (dn_ref, dnf.at[sp]), (ow_ref.at[:, mine], oww.at[tp]), (on_ref.at[:, mine], ownr.at[tp]),
        (gain_ref, gains.at[tp]), (res_hbm, res_ref), (taps_hbm, taps_ref),
    ]

    def load(index):
        src, dst = loads[index]
        return pltpu.make_async_copy(src, dst, local.at[index])

    for index in range(len(loads)):
        load(index).start()

    barrier = pltpu.get_barrier_semaphore()
    talk = [place.device(f, s) for f, s in ((1, 0), (3, 0), (0, 1), (0, 3))]
    talk += [{"sp": sp, "tp": lax.rem(tp + d, N_TP)} for d in range(1, N_TP)]
    talk += [{"sp": lax.rem(sp + d, N_SP), "tp": tp} for d in (1, N_SP - 1)]
    for device in talk:
        pl.semaphore_signal(barrier, inc=1, device_id=device, device_id_type=MESH)

    for index in range(4):
        load(index).wait()
    for half in range(2):
        floats = lraw[half * 320 : half * 320 + 320, :].astype(F32)
        mean = jnp.sum(floats * floats, axis=1, keepdims=True) * (1.0 / RANK)
        latb[half, 0] = (floats * lax.rsqrt(mean + epsilon) * lgain[...]).astype(BF16)
    position = (lax.broadcasted_iota(jnp.int32, (32, ROWS), 1) + sp * ROWS).astype(F32)
    angles = position * inv_ref[...]
    cosine, sine = jnp.cos(angles), jnp.sin(angles)

    def turn(floats):
        lower, upper = floats[0:32], floats[32:64]
        return [lower * cosine - upper * sine, lower * sine + upper * cosine]

    turned = turn(rraw[...].astype(F32))
    doubled = jnp.transpose(jnp.concatenate(turned + turned, axis=0))
    lane = lax.broadcasted_iota(jnp.int32, (160, 128), 1)
    for half in range(2):
        start = half * 320
        ropb[half, 0] = jnp.where(lane < 64, doubled[start : start + 160], doubled[start + 160 : start + 320]).astype(BF16)

    pl.semaphore_wait(barrier, len(talk))

    def lat_rows(half, target):
        if target[1] == 0:
            return half_rows(half, 320)
        start = lax.rem(place.x, 2) * (320 - PLANE)
        if half is None:
            return pl.ds(pl.multiple_of(start, 16), PLANE)
        return pl.ds(pl.multiple_of(start + half * (PLANE // 2), 16), PLANE // 2)

    def lat_view(offset, half, target):
        slot = SLOT[offset]
        return [latb.at[c, slot, lat_rows(half, target)], ropb.at[c, slot, half_rows(half, 160)]]

    def side_rows(slot, index, sent):
        parity = lax.rem(place.x + (0 if sent else 1), 2)
        start = parity * PLANE + index * (160 - PLANE // 2)
        return latb.at[c, slot, pl.ds(pl.multiple_of(start, 16), 160 - PLANE // 2)]

    lat_gather = Gather(copies, place, lat_view, ls, lr)

    def up_view(offset, half, target):
        return [upf.at[place.along(*offset), half_rows(half, 2 * UNITS)]]

    def dn_view(offset, half, target):
        return [dnf.at[place.along(*offset), half_rows(half, UNITS)]]

    up_gather = GatherPlaced(copies, place, up_view, us, ur)
    dn_gather = GatherPlaced(copies, place, dn_view, ds_, dr)

    lat_gather.forward((0, 0), lambda move: move[3][1] == 0)

    def exchange(d, start):
        to, source = lax.rem(tp + d, N_TP), lax.rem(tp + N_TP - d, N_TP)
        theirs = pl.ds(pl.multiple_of(to * FEATS, FEATS), FEATS)
        arrays = (
            (ow_ref.at[:, theirs], oww.at[tp], oww.at[source]),
            (on_ref.at[:, theirs], ownr.at[tp], ownr.at[source]),
            (gain_ref, gains.at[tp], gains.at[source]),
        )
        for index, (src, dst, landed) in enumerate(arrays):
            if start:
                copies.start(
                    lambda src=src, dst=dst, index=index: (
                        src, dst, xs.at[index, d], xr.at[index, d], {"sp": sp, "tp": to}
                    )
                )
            else:
                copies.arrived(landed, xr.at[index, d], {"sp": sp, "tp": to})

    for d in range(1, N_TP):
        exchange(d, True)

    for index in (4, 5):
        load(index).wait()
    blank = jnp.zeros((64, ROWS), F32)
    rope_part = [SCALE_W * piece for piece in turn(qt[128:192, :].astype(F32))]
    qw_ref[:, 0:128] = jnp.transpose(qt[0:128, :].astype(F32)).astype(BF16)
    qw_ref[:, 128:256] = jnp.transpose(jnp.concatenate([blank] + rope_part, axis=0)).astype(BF16)
    narrow_query = jnp.transpose(qraw[...].astype(F32))
    rope_part = [SCALE_N * piece for piece in turn(narrow_query[64:128])]
    qn_ref[...] = jnp.transpose(jnp.concatenate([narrow_query[0:64]] + rope_part, axis=0)).astype(BF16)
    for index in (6, 7):
        load(index).wait()

    mrow[...] = jnp.full_like(mrow, -1e30)
    acc[...] = jnp.zeros_like(acc)

    def partner_view(core, slot):
        return [latb.at[core, slot], ropb.at[core, slot]]

    def weights_at(point):
        for name in PLAN.get(point, "").split():
            gather, step = (up_gather, dn_gather)[name[0] == "D"], int(name[1])
            if step == 0:
                for index in (8, 9) if name[0] == "U" else (10,):
                    load(index).wait()
            for offset in STEPS[step]:
                gather.wait(offset)
                gather.forward(offset)

    def across(offset):
        slot = SLOT[offset]
        for index in range(2):
            copies.start(
                lambda index=index: (
                    partner_view(c, slot)[index], partner_view(c, slot)[index],
                    lps.at[index, slot], lpr.at[index, slot], place.peer(0, 1),
                )
            )

    def plane_arrival(offset):
        slot = SLOT[offset]
        lat_gather.wait(offset)
        lat_gather.forward(offset)
        if offset[1] == 0:
            across(offset)
            return
        for index, dx in enumerate((1, 3)):
            copies.start(
                lambda index=index, dx=dx: (
                    side_rows(slot, index, True), side_rows(slot, index, True),
                    xls.at[index, slot], xlr.at[index, slot], place.peer(dx),
                )
            )

    def side_arrival(offset):
        slot = SLOT[offset]
        for index in range(2):
            copies.arrived(side_rows(slot, index, False), xlr.at[index, slot], place.peer(1))
        across(offset)

    def partner_arrival(offset):
        slot = SLOT[offset]
        for index, ref in enumerate(partner_view(1 - c, slot)):
            copies.arrived(ref, lpr.at[index, slot], place.peer(0, 1))

    def take(point):
        for name in SCHEDULE.get(point, "").split():
            pair = int(name[1:])
            if name[0] == "E":
                for offset in TAKEN[name]:
                    plane_arrival(offset)
            else:
                for offset in ORDER[2 * pair : 2 * pair + 2]:
                    (side_arrival if name[0] == "X" else partner_arrival)(offset)
        weights_at(point)

    def expand(pair, side):
        lane = lax.broadcasted_iota(jnp.int32, (160, 128), 1)
        for u in range(4):
            block = latb[u % 2, 2 * pair + u // 2]
            rope = ropb[u % 2, 2 * pair + u // 2].astype(F32)
            wide = jnp.dot(block, ew_ref[...], preferred_element_type=F32)
            narrow = jnp.dot(block, en_ref[...], preferred_element_type=F32)
            rows = pl.ds(u * 320, 320)
            kbuf[side, rows, 0:128] = (wide[:, :128] * SCALE_W).astype(BF16)
            vbuf[side, rows, 0:128] = wide[:, 128:].astype(BF16)
            scaled = narrow * SCALE_N
            kbuf[side, pl.ds(u * 320, 160), 128:256] = jnp.where(
                lane < 64, scaled[:160], pltpu.roll(rope, 64, 1)
            ).astype(BF16)
            kbuf[side, pl.ds(u * 320 + 160, 160), 128:256] = jnp.where(lane < 64, scaled[160:], rope).astype(BF16)
            for row in (0, 160):
                vbuf[side, pl.ds(u * 320 + row, 160), 128:256] = jnp.where(lane < 64, 1.0, narrow[row : row + 160]).astype(
                    BF16
                )

    def score(group, side):
        q_ref, lanes = (qw_ref, slice(0, 256)) if group == 0 else (qn_ref, slice(128, 256))
        sbuf[group] = lax.dot_general(
            q_ref[...], kbuf[side, :, lanes], (((1,), (1,)), ((), ())), preferred_element_type=F32
        )

    def soften(group):
        for start in range(0, ROWS, CHUNK):
            rows = slice(start, start + CHUNK)
            kept = slice(group * ROWS + start, group * ROWS + start + CHUNK)
            scores = sbuf[group, rows, :]
            before = mrow[kept, :]
            top = jnp.maximum(before, jnp.max(scores, axis=1, keepdims=True))
            mrow[kept, :] = top
            pbuf[group, rows, :] = jnp.exp2(scores - top[:, 0:1]).astype(BF16)
            shrink = jnp.exp2(before - top)
            acc[kept, 0:128] = shrink * acc[kept, 0:128]
            if group == 0:
                acc[kept, 128:256] = shrink * acc[kept, 128:256]

    def gain_values(group, side):
        if group == 0:
            acc[0:ROWS, :] += jnp.dot(pbuf[0], vbuf[side], preferred_element_type=F32)
        else:
            acc[ROWS : 2 * ROWS, 0:128] += jnp.dot(pbuf[1], vbuf[side, :, 128:256], preferred_element_type=F32)

    pbuf[1] = jnp.zeros_like(pbuf[1])
    vbuf[1] = jnp.zeros_like(vbuf[1])
    for offset, half in (((3, 0), 0), ((1, 0), 1)):
        lat_gather.wait(offset, (half,))
        lat_gather.forward(offset, lambda move: move[3] == (2, 0))
    lat_gather.forward((0, 0), lambda move: move[3][1] != 0)
    for offset, half in (((1, 0), 0), ((3, 0), 1)):
        lat_gather.wait(offset, (half,))
        lat_gather.forward(offset, lambda move: move[3] != (2, 0))
        across(offset)
    partner_arrival((1, 0))
    expand(0, 0)
    score(0, 0)

    def attention_step(pair, carry):
        side = lax.rem(pair, 2)
        for k in range(PAIRS - 1):

            @pl.when(pair == k)
            def _():
                take(f"s{k}")

        score(1, side)
        gain_values(1, 1 - side)
        soften(0)
        for k in range(PAIRS - 1):

            @pl.when(pair == k)
            def _():
                take(f"m{k}")

        expand(pair + 1, 1 - side)
        gain_values(0, side)
        score(0, 1 - side)
        soften(1)
        return carry

    lax.fori_loop(0, PAIRS - 1, attention_step, 0)
    weights_at("last")
    last = (PAIRS - 1) % 2
    score(1, last)
    gain_values(1, 1 - last)
    soften(0)
    gain_values(0, last)
    hw[tp] = (acc[0:ROWS, 0:128] / acc[0:ROWS, 128:129]).astype(BF16)
    head_gather = RingGather(
        copies,
        place,
        lambda feature, half: [hw.at[feature, half_rows(half, 640)], hn.at[feature, half_rows(half, 320)]],
        hs,
        hr,
    )
    head_gather.begin((0,))
    soften(1)
    gain_values(1, last)

    low = acc[ROWS : ROWS + 320, 0:128] / acc[ROWS : ROWS + 320, 0:1]
    high = acc[ROWS + 320 : 2 * ROWS, 0:128] / acc[ROWS + 320 : 2 * ROWS, 0:1]
    lane = lax.broadcasted_iota(jnp.int32, (320, 128), 1)
    hn[tp] = jnp.where(lane < 64, pltpu.roll(low, 64, 1), high).astype(BF16)
    head_gather.begin((1,))

    weights_at("heads")

    for d in range(1, N_TP):
        exchange(d, False)
    for index in range(11, 16):
        load(index).wait()
    zero = jnp.zeros((64, FEATS), BF16)
    for j in range(N_TP):
        own0[pl.ds(j * 128, 64), :] = ownr[j]
        own0[pl.ds(j * 128 + 64, 64), :] = zero
        own1[pl.ds(j * 128, 64), :] = zero
        own1[pl.ds(j * 128 + 64, 64), :] = ownr[j]

    head_gather.middle()
    weights_at("middle")
    head_gather.end()
    weights_at("ended")

    wide_heads = jnp.concatenate([hw[j] for j in range(N_TP)], axis=1)
    narrow_heads = jnp.concatenate([hn[j] for j in range(N_TP)], axis=1)
    summed = jnp.dot(wide_heads, oww[...].reshape(N_TP * 128, FEATS), preferred_element_type=F32)
    top = jnp.dot(narrow_heads, own0[...], preferred_element_type=F32)
    bottom = jnp.dot(narrow_heads, own1[...], preferred_element_type=F32)
    att[tp, 0:320] = (res_ref[0:320, :].astype(F32) + summed[0:320] + top).astype(BF16)
    att[tp, 320:640] = (res_ref[320:640, :].astype(F32) + summed[320:640] + bottom).astype(BF16)

    att_gather = RingGather(
        copies, place, lambda feature, half: [att.at[feature, half_rows(half, 640)]], as_, ar
    )
    att_gather.begin()
    weights_at("begin")
    att_gather.middle()
    weights_at("joined")
    att_gather.end()
    weights_at("full")

    def norm_step(index, carry):
        rows = pl.ds(index * 64, 64)
        squares = jnp.zeros((64, FEATS), F32)
        for j in range(N_TP):
            piece = att[j, rows, :].astype(F32)
            squares = squares + piece * piece
        factor = lax.rsqrt(jnp.sum(squares, axis=1, keepdims=True) * (1.0 / D) + epsilon)
        for j in range(N_TP):
            nrm[rows, j * FEATS : (j + 1) * FEATS] = (
                att[j, rows, :].astype(F32) * factor * gains[j]
            ).astype(BF16)
        return carry

    lax.fori_loop(0, ROWS // 64, norm_step, 0)

    for base, dest in ((0, gx), (UNITS, vx)):
        for start in (0, 256, 512):
            stop = min(start + 256, UNITS)
            weights = jnp.concatenate([upf[o, base + start : base + stop, :] for o in range(N_SP)], axis=1)
            dest[EDGE : EDGE + ROWS, start:stop] = lax.dot_general(
                nrm[...], weights, (((1,), (1,)), ((), ())), preferred_element_type=F32
            ).astype(BF16)

    weights_at("up")
    following = {"sp": lax.rem(sp + 1, N_SP), "tp": tp}
    leading = {"sp": lax.rem(sp + N_SP - 1, N_SP), "tp": tp}
    edges = [
        (rows, landing, 2 * index + side, device)
        for side, (rows, landing, device) in enumerate(((ROWS, 0, following), (EDGE, ROWS + EDGE, leading)))
        for index in range(2)
    ]

    def edge(rows, landing, index, device):
        ref = (gx, vx)[index // 2]
        return ref.at[pl.ds(rows, EDGE)], ref.at[pl.ds(landing, EDGE)], es.at[index], er.at[index], device

    for entry in edges:
        copies.start(lambda entry=entry: edge(*entry))
    weights_at("edge")

    def conv_step(index, place_of):
        span = pl.ds(index * 128, 160)
        position = lax.broadcasted_iota(jnp.int32, (160, 1), 0) + index * 128 - EDGE
        outside = ((sp == 0) & (position < 0)) | ((sp == N_SP - 1) & (position >= ROWS))

        def smooth(ref, which, columns):
            wide = jnp.where(outside, 0.0, ref[span, columns].astype(F32))
            low = pltpu.roll(wide, 1, 0)[16:144]
            high = pltpu.roll(wide, 159, 0)[16:144]
            taps = [taps_ref[k, which : which + 1, columns] for k in range(3)]
            return taps[0] * low + taps[1] * wide[16:144] + taps[2] * high

        rows = pl.ds(place_of * 128, 128)
        for start in range(0, UNITS, 128):
            columns = slice(start, min(start + 128, UNITS))
            gate = smooth(gx, 0, columns)
            value = smooth(vx, 1, columns)
            hid[rows, columns] = (gate / (1.0 + jnp.exp(-gate)) * value).astype(BF16)

    def inner_step(index, carry):
        conv_step(index, index - 1)
        return carry

    lax.fori_loop(1, 4, inner_step, 0)

    def down(feature, rows):
        weights = jnp.concatenate([dnf[2 * feature], dnf[2 * feature + 1]], axis=1)
        return jnp.dot(hid[rows, :], weights, preferred_element_type=F32)

    class Reduce:
        def __init__(self, start, count, first):
            self.rows = slice(start, start + count)
            self.halves = (slice(start, start + count // 2), slice(start + count // 2, start + count))
            self.first = first

        def move(self, ref, other, index, device):
            index += self.first
            copies.start(lambda: (ref(), other(), rs.at[index], rr.at[index], device()))

        def landed(self, ref, index):
            copies.arrived(ref, rr.at[index + self.first], place.peer(1))

        def down_pair(self, dx):
            rows = self.rows
            send_a[dx, rows] = down(place.feature(dx, 1), rows).astype(BF16)
            self.move(lambda: send_a.at[dx, rows], lambda: recv_a.at[dx, rows], dx, lambda: place.peer(0, 1))
            part[dx, rows] = down(place.feature(dx), rows)

        def pair_sum(self, dx):
            self.landed(recv_a.at[dx, self.rows], dx)
            return part[dx, self.rows] + recv_a[dx, self.rows].astype(F32)

        def far(self):
            total = self.pair_sum(2).astype(BF16)
            for side, rows in enumerate(self.halves):
                send_b[rows] = total[rows.start - self.rows.start : rows.stop - self.rows.start]
                self.move(
                    lambda rows=rows: send_b.at[rows], lambda rows=rows: recv_b.at[rows], 4 + side,
                    lambda side=side: place.peer((1, 3)[side]),
                )

        def near(self, side):
            total = self.pair_sum((1, 3)[side])
            part[(1, 3)[side], self.rows] = total
            rows = self.halves[1 - side]
            send_c[side, rows] = total[rows.start - self.rows.start : rows.stop - self.rows.start].astype(BF16)
            self.send(side, rows, 6 + side)

        def send(self, side, rows, index):
            self.move(
                lambda: send_c.at[side, rows], lambda: recv_c.at[side, rows], index, lambda: place.peer((1, 3)[side])
            )

        def join(self):
            for side, rows in enumerate(self.halves):
                self.landed(recv_b.at[rows], 4 + side)
                send_c[side, rows] = (part[(1, 3)[side], rows] + recv_b[rows].astype(F32)).astype(BF16)
                self.send(side, rows, 8 + side)

        def result(self):
            total = self.pair_sum(0)
            for side in range(2):
                self.landed(recv_c.at[side, self.halves[1 - side]], 6 + side)
                self.landed(recv_c.at[side, self.halves[side]], 8 + side)
            return total + recv_c[0, self.rows].astype(F32) + recv_c[1, self.rows].astype(F32)

    first, second = Reduce(0, 384, 0), Reduce(384, 256, 10)
    first.down_pair(2)
    first.down_pair(1)
    first.far()
    first.down_pair(3)
    first.near(0)
    first.down_pair(0)
    first.near(1)
    for rows, landing, index, device in edges:
        copies.arrived(edge(rows, landing, index, device)[1], er.at[index], device)
    conv_step(0, 3)
    conv_step(4, 4)
    second.down_pair(2)
    second.down_pair(1)
    second.far()
    second.down_pair(3)
    second.near(0)
    first.join()
    second.down_pair(0)
    second.near(1)
    second.join()
    out_ref[128:512, :] = (att[tp, 128:512].astype(F32) + first.result()).astype(BF16)
    rest = second.result()
    out_ref[0:128, :] = (att[tp, 0:128].astype(F32) + rest[0:128]).astype(BF16)
    out_ref[512:640, :] = (att[tp, 512:640].astype(F32) + rest[128:256]).astype(BF16)
    copies.drain()


def per_device(
    residual, query_wide, query_narrow, latent, rope_key, latent_gain, expand_wide, expand_narrow,
    out_wide, out_narrow, norm_gain, up_gate, up_value, down_weight, conv_taps,
):
    inverse = np.power(np.float32(theta), -2.0 * np.arange(32, dtype=np.float32) / ROPE).astype(np.float32)
    inverse = jnp.asarray(inverse[:, None])
    vmem = pl.BlockSpec(memory_space=pltpu.VMEM)
    anywhere = pl.BlockSpec(memory_space=pl.ANY)
    dma = pltpu.SemaphoreType.DMA
    return pl.pallas_call(
        kernel,
        out_shape=jax.ShapeDtypeStruct((ROWS, FEATS), BF16),
        in_specs=[anywhere] * 16,
        out_specs=vmem,
        scratch_shapes=[
            pltpu.VMEM((2, 16, 320, RANK), BF16),
            pltpu.VMEM((2, 16, 160, 128), BF16),
            pltpu.VMEM((N_SP, 2 * UNITS, 128), BF16),
            pltpu.VMEM((N_SP, UNITS, 128), BF16),
            pltpu.VMEM((2, KEYS, 256), BF16),
            pltpu.VMEM((2, KEYS, 256), BF16),
            pltpu.VMEM((2, ROWS, KEYS), F32),
            pltpu.VMEM((2, ROWS, KEYS), BF16),
            pltpu.VMEM((2 * ROWS, 128), F32),
            pltpu.VMEM((2 * ROWS, 256), F32),
            pltpu.VMEM((N_TP, ROWS, 128), BF16),
            pltpu.VMEM((N_TP, ROWS // 2, 128), BF16),
            pltpu.VMEM((N_TP, 128, FEATS), BF16),
            pltpu.VMEM((N_TP, 64, FEATS), BF16),
            pltpu.VMEM((N_TP * 128, FEATS), BF16),
            pltpu.VMEM((N_TP * 128, FEATS), BF16),
            pltpu.VMEM((N_TP, 1, FEATS), F32),
            pltpu.VMEM((N_TP, ROWS, FEATS), BF16),
            pltpu.VMEM((ROWS, D), BF16),
            pltpu.VMEM((ROWS + 2 * EDGE, UNITS), BF16),
            pltpu.VMEM((ROWS + 2 * EDGE, UNITS), BF16),
            pltpu.VMEM((ROWS, UNITS), BF16),
            pltpu.VMEM((4, ROWS, FEATS), F32),
            pltpu.VMEM((4, ROWS, FEATS), BF16),
            pltpu.VMEM((4, ROWS, FEATS), BF16),
            pltpu.VMEM((ROWS, FEATS), BF16),
            pltpu.VMEM((ROWS, FEATS), BF16),
            pltpu.VMEM((2, ROWS, FEATS), BF16),
            pltpu.VMEM((2, ROWS, FEATS), BF16),
            pltpu.VMEM((NOPE_W + ROPE, ROWS), BF16),
            pltpu.VMEM((ROWS, 128), BF16),
            pltpu.VMEM((ROWS, 256), BF16),
            pltpu.VMEM((ROWS, 128), BF16),
            pltpu.VMEM((ROWS, RANK), BF16),
            pltpu.VMEM((ROPE, ROWS), BF16),
            pltpu.VMEM((1, RANK), F32),
            pltpu.VMEM((RANK, 256), BF16),
            pltpu.VMEM((RANK, 128), BF16),
            pltpu.VMEM((ROWS, FEATS), BF16),
            pltpu.VMEM((3, 2, UNITS), F32),
            pltpu.VMEM((32, 1), F32),
            dma((2, N_SEND)), dma((2, 32)), dma((2, 16)), dma((2, 16)), dma((2, 16)), dma((2, 16)),
            dma((1, N_SEND)), dma((1, 32)),
            dma((1, N_SEND)), dma((1, 32)),
            dma((2, 10)), dma((2, 10)),
            dma((1, 10)), dma((1, 10)),
            dma((3, 8)), dma((3, 8)),
            dma((4,)), dma((4,)),
            dma((20,)), dma((20,)),
            dma((16,)),
        ],
        compiler_params=pltpu.CompilerParams(
            collective_id=0, has_side_effects=True, vmem_limit_bytes=67043328
        ),
    )(
        query_wide.T, query_narrow, latent, rope_key.T, latent_gain.reshape(1, RANK), expand_wide, expand_narrow,
        residual, out_wide, out_narrow, norm_gain.reshape(1, FEATS), up_gate.T, up_value.T, down_weight.T, conv_taps, inverse,
    )


def solution(mesh):
    in_specs = (
        P("sp", "tp"), P("sp", "tp"), P("sp", "tp"), P("sp", None), P("sp", None), P(),
        P(None, "tp"), P(None, "tp"), P("tp", None), P("tp", None), P("tp"),
        P("sp", "tp"), P("sp", "tp"), P("sp", "tp"), P(None, None, "tp"),
    )
    return jax.shard_map(
        per_device, mesh=mesh, in_specs=in_specs, out_specs=P("sp", "tp"), check_vma=False
    )
```
